128 devices in a mesh: ep: 16 (over z, x), tp: 8 (over y, core).
Axes of the slice: x: 4, y: 4, z: 4, core: 2. Of those that a mesh axis runs over, the one named last changes fastest.
Arguments:
- residual: bfloat16 [2048, 2048], P('ep', 'tp'), may hold values from -61 to 61
- in_gain: float32 [2048], replicated, may hold values from 0.1 to 1.9
- in_weight: bfloat16 [2048, 1024], P(None, 'tp'), may hold values from -0.125 to 0.125
- state: float32 [2, 2048, 4096], P(None, 'ep', 'tp'), may hold values from -3 to 3
- decay_rate: float32 [64, 64], P('tp'), may hold values from 0.1 to 1
- frequency: float32 [64, 64], P('tp'), may hold values from 0 to 200
- log_step: float32 [64], P('tp'), may hold values from -3 to -0.7
- in_coef: float32 [2, 64, 64, 16], P(None, 'tp'), may hold values from -1 to 1
- out_coef: float32 [2, 64, 16, 64], P(None, 'tp'), may hold values from -0.75 to 0.75
- skip_gain: float32 [1024], P('tp'), may hold values from -3 to 3
- out_weight: bfloat16 [1024, 2048], replicated, may hold values from -0.1875 to 0.1875
- mid_gain: float32 [2048], replicated, may hold values from 0.1 to 1.9
- gate_vector: bfloat16 [2048], replicated, may hold values from -0.125 to 0.125
- routes: int32 [2048, 4], P('ep'), may hold values from 0 to 127, all different within a row; in each aligned block of 128 rows (0 to 127, 128 to 255, ...) at most 8 rows name the same one
- route_weight: float32 [2048, 4], P('ep'), may hold values from 0.1 to 1
- expert_gate: bfloat16 [128, 2048, 512], P(('ep', 'tp')), may hold values from -0.125 to 0.125
- expert_up: bfloat16 [128, 2048, 512], P(('ep', 'tp')), may hold values from -0.125 to 0.125
- expert_down: bfloat16 [128, 512, 2048], P(('ep', 'tp')), may hold values from -0.25 to 0.25
- shared_gate: bfloat16 [2048, 4096], P(None, 'ep'), may hold values from -0.125 to 0.125
- shared_up: bfloat16 [2048, 4096], P(None, 'ep'), may hold values from -0.125 to 0.125
- shared_down: bfloat16 [4096, 2048], P('ep'), may hold values from -0.09375 to 0.09375
Outputs:
- layer_out: bfloat16 [2048, 2048], P(('ep', 'tp'))
- new_state: float32 [2, 2048, 4096], P(None, 'ep', 'tp')
The draws below stay inside these ranges and needn't reach their ends.
Inputs may be any that keep to these rules, and one draw needn't show every extreme that they name: `routes`: each row names 4 different experts. Among the rows of one index of ep no expert is named more than 8 times, a bound that some block reaches.
All inputs are finite; a program needn't handle non-finite values.
Results may differ from the reference program's by a relative error of at most 0.0085.
Values may be sent and summed in bfloat16 or wider, within the bound.
No kernel may reach another device: no remote copies, remote signals or barrier semaphores. Data moves between devices by JAX's collectives and lax.ppermute only.
A program may use at most 128 MiB of HBM per device.

```python
import math
import jax
import jax.numpy as jnp
import numpy as np
from jax import lax

D = 2048
SW = 1024
GROUP_CH = 16
STATE = 64
GROUPS = 64
GS = 4096
FF = 512
SFF = 4096
TOP = 4
SEQ_DEV = 128
SEQS = 2048
EXPERTS = 128
CAP = 8
N_EP = 16


def draw_residual(key, part):
    first_key, second_key = jax.random.split(jax.random.fold_in(key, 11))
    columns = jnp.arange(D, dtype=jnp.float32)
    col_scale = 10.0 ** (columns / D - 0.5)
    row_scale = 10.0 ** jax.random.uniform(second_key, (SEQS, 1), jnp.float32, -0.5, 0.5)
    base_draw = jnp.clip(jax.random.normal(first_key, (SEQS, D), jnp.float32), -6.0, 6.0)
    return (base_draw * col_scale * row_scale).astype(jnp.bfloat16)


def levels(stream_key, shape, cuts, low, high):
    def one(axis_at, blocks):
        draws = jax.random.uniform(jax.random.fold_in(jax.random.fold_in(stream_key, 6), axis_at), (blocks,), jnp.float32, low / len(cuts), high / len(cuts))
        return jnp.repeat(jnp.exp(draws), shape[axis_at] // blocks).reshape((-1,) + (1,) * (len(shape) - axis_at - 1))

    gain = one(*cuts[0])
    for cut in cuts[1:]:
        gain = gain * one(*cut)
    return gain


def deal_out(stream_key, own, number, rows, number_of, top, most, slope):
    order = jax.random.permutation(stream_key, number_of)
    crowded, common = load_shares(number_of, rows * top, most, slope, True), load_shares(number_of, rows * top, most, slope, False)
    places = jnp.arange(number_of)

    def named(sizes, offset_by):
        used = int((sizes > 0).sum())
        fixed = max(1, used // 4)
        moved = fixed + (places - fixed + offset_by * (used - fixed)) % max(1, number_of - fixed)
        return jnp.zeros((number_of,), jnp.int32).at[order[jnp.where(places < fixed, places, moved)]].set(jnp.asarray(sizes, jnp.int32))

    sizes = jnp.where(number % 4 == 0, named(crowded, number // 4), named(common, number - number // 4 - 1))
    mixed = jax.random.permutation(jax.random.fold_in(own, 3), number_of)
    giver, receiver = mixed[0:number_of // 2 * 2:2], mixed[1:number_of // 2 * 2:2]
    room = jnp.minimum(sizes[giver] - 1, most - sizes[receiver]) // 2
    room = jnp.where((giver == order[0]) | (receiver == order[0]) | (sizes[receiver] == 0), 0, jnp.maximum(room, 0))
    moved = jax.random.randint(jax.random.fold_in(own, 4), (number_of // 2,), 0, 1 << 20) % (room + 1)
    sizes = sizes.at[giver].add(-moved).at[receiver].add(moved)
    labels = jnp.searchsorted(jnp.cumsum(sizes), jnp.arange(rows * top), side="right").astype(jnp.int32)
    grid = labels.reshape(top, rows).T
    grid = grid[jax.random.permutation(jax.random.fold_in(own, 1), rows)]
    offset_by = jax.random.randint(jax.random.fold_in(own, 2), (rows, 1), 0, top)
    return jnp.take_along_axis(grid, (jnp.arange(top)[None, :] + offset_by) % top, axis=1)


def load_shares(amount, total, bound, lean, full):
    loads = [(1 << 20) // math.isqrt(standing ** lean) + 1 for standing in range(1, amount + 1)]
    largest = bound if full else min(bound, max(-(-total // amount), total * loads[0] // sum(loads)))
    least = 1 if total - largest >= amount - 1 else 0
    holding, spare = [largest] + [least] * (amount - 1), total - largest - least * (amount - 1)
    while spare > 0:
        free = [i for i in range(1, amount) if holding[i] < largest] or [i for i in range(1, amount) if holding[i] < bound]
        pool, left = sum([loads[i] for i in free]), spare
        for i in free:
            extra = min(bound - holding[i], max(1, left * loads[i] // pool), spare)
            holding[i] = holding[i] + extra
            spare = spare - extra
    return np.array(holding)


def noise(stream_key, dims, deviation, limit, pieces=(), kind=jnp.bfloat16):
    drawn = deviation * jax.random.normal(stream_key, dims, jnp.float32)
    if pieces:
        drawn = drawn * levels(stream_key, dims, pieces, -0.22, 0.18)
    return jnp.clip(drawn, -limit, limit).astype(kind)


def setup_inputs(seed: int = 0) -> dict:
    seeds = jax.random.split(jax.random.key(seed), 22)
    residual = draw_residual(jax.random.fold_in(seeds[21], 71), 0)
    in_gain = jnp.clip(1.0 + 0.18 * jax.random.normal(seeds[1], (D,), jnp.float32), 0.1, 1.9)
    in_weight = noise(seeds[2], (D, SW), D ** -0.5, 0.125, ((1, 8),))
    state = noise(seeds[3], (2, SEQS, GS), 0.5, 3.0, ((1, 16), (2, 8)), jnp.float32)
    decay_rate = jnp.clip(jnp.exp(math.log(1.0) - 2.3025851 * jax.random.uniform(seeds[4], (GROUPS, STATE), jnp.float32) ** levels(seeds[4], (GROUPS, STATE), ((0, 8),), -0.2, 0.2)), 0.1, 1.0)
    frequency = jnp.clip(200.0 * jax.random.uniform(seeds[5], (GROUPS, STATE), jnp.float32) ** levels(seeds[5], (GROUPS, STATE), ((0, 8),), -0.2, 0.2), 0.0, 200.0)
    log_step = jnp.clip(-3.0 + 2.3 * jax.random.uniform(seeds[6], (GROUPS,), jnp.float32) ** levels(seeds[6], (GROUPS,), ((0, 8),), -0.2, 0.2), -3.0, -0.7)
    in_coef = noise(seeds[7], (2, GROUPS, STATE, GROUP_CH), (2 * GROUP_CH) ** -0.5, 1.0, ((1, 8),), jnp.float32)
    out_coef = noise(seeds[8], (2, GROUPS, GROUP_CH, STATE), STATE ** -0.5, 0.75, ((1, 8),), jnp.float32)
    skip_gain = noise(seeds[9], (SW,), 0.5, 3.0, ((0, 8),), jnp.float32)
    out_weight = noise(seeds[10], (SW, D), SW ** -0.5, 0.1875)
    mid_gain = jnp.clip(1.0 + 0.18 * jax.random.normal(seeds[11], (D,), jnp.float32), 0.1, 1.9)
    gate_vector = noise(seeds[12], (D,), D ** -0.5, 0.125)
    routes_keys = jax.random.split(jax.random.fold_in(seeds[13], 1), SEQS // SEQ_DEV)
    routes_turns = jax.random.permutation(jax.random.fold_in(seeds[13], 3), SEQS // SEQ_DEV)
    routes = jax.vmap(lambda own, number: deal_out(jax.random.fold_in(seeds[13], 2), own, number, SEQ_DEV, EXPERTS, TOP, CAP, 2))(routes_keys, routes_turns).reshape((SEQS, TOP))
    route_weight = jnp.clip(jnp.exp(math.log(1.0) - 2.3025851 * jax.random.uniform(seeds[14], (SEQS, TOP), jnp.float32) ** levels(seeds[14], (SEQS, TOP), ((0, 16),), -0.2, 0.2)), 0.1, 1.0)
    expert_gate = noise(seeds[15], (EXPERTS, D, FF), D ** -0.5, 0.125, ((0, 128),))
    expert_up = noise(seeds[16], (EXPERTS, D, FF), D ** -0.5, 0.125, ((0, 128),))
    expert_down = noise(seeds[17], (EXPERTS, FF, D), FF ** -0.5, 0.25, ((0, 128),))
    shared_gate = noise(seeds[18], (D, SFF), D ** -0.5, 0.125, ((1, 16),))
    shared_up = noise(seeds[19], (D, SFF), D ** -0.5, 0.125, ((1, 16),))
    shared_down = noise(seeds[20], (SFF, D), SFF ** -0.5, 0.09375, ((0, 16),))
    return dict(residual=residual, in_gain=in_gain, in_weight=in_weight, state=state, decay_rate=decay_rate, frequency=frequency, log_step=log_step, in_coef=in_coef, out_coef=out_coef, skip_gain=skip_gain, out_weight=out_weight, mid_gain=mid_gain, gate_vector=gate_vector, routes=routes, route_weight=route_weight, expert_gate=expert_gate, expert_up=expert_up, expert_down=expert_down, shared_gate=shared_gate, shared_up=shared_up, shared_down=shared_down)


norm_eps = 1e-05
routed_scale = 2.5

def layer_norm(values, gain_vec):
    row_mean = lax.optimization_barrier(jnp.mean(values, axis=-1, keepdims=True))
    row_square = lax.optimization_barrier(jnp.mean(values * values, axis=-1, keepdims=True))
    return (values - row_mean) * lax.rsqrt(row_square - row_mean * row_mean + norm_eps) * gain_vec.astype(jnp.float32)

def coefficients(decay_rate, frequency, log_step, in_coef):
    time_step = jnp.exp(log_step)[:, None]
    real_rate = -decay_rate
    magnitude = jnp.exp(real_rate * time_step)
    keep_re = magnitude * jnp.cos(frequency * time_step)
    keep_im = magnitude * jnp.sin(frequency * time_step)
    denominator = real_rate * real_rate + frequency * frequency
    factor_re = ((keep_re - 1.0) * real_rate + keep_im * frequency) / denominator
    factor_im = (keep_im * real_rate - (keep_re - 1.0) * frequency) / denominator
    push_re = factor_re[..., None] * in_coef[0] - factor_im[..., None] * in_coef[1]
    push_im = factor_re[..., None] * in_coef[1] + factor_im[..., None] * in_coef[0]
    return (keep_re, keep_im, push_re, push_im)

def mixer_step(normed, in_weight, state, decay_rate, frequency, log_step, in_coef, out_coef, skip_gain):
    row_count = normed.shape[0]
    group_count, state_count = decay_rate.shape
    keep_re, keep_im, push_re, push_im = coefficients(decay_rate, frequency, log_step, in_coef)
    drive = jnp.dot(normed, in_weight, preferred_element_type=jnp.float32).astype(jnp.bfloat16)
    drive_f = drive.astype(jnp.float32).reshape(row_count, group_count, -1)
    highest = lax.Precision.HIGHEST
    input_re = jnp.einsum('tgh,gph->tgp', drive_f, push_re, precision=highest)
    input_im = jnp.einsum('tgh,gph->tgp', drive_f, push_im, precision=highest)
    old_re = state[0].reshape(row_count, group_count, state_count)
    old_im = state[1].reshape(row_count, group_count, state_count)
    new_re = keep_re * old_re - keep_im * old_im + input_re
    new_im = keep_re * old_im + keep_im * old_re + input_im
    read_out = jnp.einsum('ghp,tgp->tgh', out_coef[0], new_re, precision=highest) - jnp.einsum('ghp,tgp->tgh', out_coef[1], new_im, precision=highest)
    read_out = read_out.reshape(row_count, -1) + skip_gain * drive_f.reshape(row_count, -1)
    mixed_rows = jax.nn.gelu(read_out, approximate=True).astype(jnp.bfloat16)
    updated = jnp.stack([new_re.reshape(row_count, -1), new_im.reshape(row_count, -1)])
    return (mixed_rows, updated)

def route_slots(routes, experts):
    flat_routes = routes.reshape(-1)
    onehot = (flat_routes[:, None] == jnp.arange(experts, dtype=jnp.int32)[None, :]).astype(jnp.int32)
    before = jnp.cumsum(onehot, axis=0) - onehot
    return lax.optimization_barrier(jnp.sum(before * onehot, axis=1)).reshape(routes.shape)

def expert_block(row_block, gate_weight, up_weight, down_weight):
    gate_part = jnp.dot(row_block, gate_weight, preferred_element_type=jnp.float32)
    up_part = jnp.dot(row_block, up_weight, preferred_element_type=jnp.float32)
    hidden = (jax.nn.silu(gate_part) * up_part).astype(jnp.bfloat16)
    return jnp.dot(hidden, down_weight, preferred_element_type=jnp.float32).astype(jnp.bfloat16)

def reference(residual, in_gain, in_weight, state, decay_rate, frequency, log_step, in_coef, out_coef, skip_gain, out_weight, mid_gain, gate_vector, routes, route_weight, expert_gate, expert_up, expert_down, shared_gate, shared_up, shared_down):
    resid_f = residual.astype(jnp.float32)
    normed = layer_norm(resid_f, in_gain).astype(jnp.bfloat16)
    mixed_rows, new_state = mixer_step(normed, in_weight, state, decay_rate, frequency, log_step, in_coef, out_coef, skip_gain)
    after_mix = resid_f + jnp.dot(mixed_rows, out_weight, preferred_element_type=jnp.float32)
    normed_mid = layer_norm(after_mix, mid_gain).astype(jnp.bfloat16)
    slot_rank = jax.vmap(route_slots, in_axes=(0, None))(routes.reshape(N_EP, SEQ_DEV, TOP), EXPERTS).reshape(SEQS, TOP)
    group_of = (jnp.arange(SEQS, dtype=jnp.int32) // SEQ_DEV)[:, None]
    slot_place = routes * (N_EP * CAP) + group_of * CAP + slot_rank
    token_ids = jnp.broadcast_to(jnp.arange(SEQS, dtype=jnp.int32)[:, None], slot_place.shape)
    slot_token = jnp.zeros((EXPERTS * N_EP * CAP,), jnp.int32).at[slot_place.reshape(-1)].set(token_ids.reshape(-1))
    buffer = normed_mid[slot_token].reshape(EXPERTS, N_EP * CAP, D)
    outputs = lax.map(lambda packed: expert_block(*packed), (buffer, expert_gate, expert_up, expert_down)).reshape(EXPERTS * N_EP * CAP, D)
    weights = route_weight / lax.optimization_barrier(jnp.sum(route_weight, axis=-1, keepdims=True)) * routed_scale
    routed = lax.optimization_barrier(jnp.sum(weights[..., None] * outputs[slot_place].astype(jnp.float32), axis=1))
    gate_part = jnp.dot(normed_mid, shared_gate, preferred_element_type=jnp.float32)
    up_part = jnp.dot(normed_mid, shared_up, preferred_element_type=jnp.float32)
    shared_hidden = (jax.nn.silu(gate_part) * up_part).astype(jnp.bfloat16)
    shared = jnp.dot(shared_hidden, shared_down, preferred_element_type=jnp.float32)
    gate_value = jax.nn.sigmoid(jnp.dot(normed_mid, gate_vector, preferred_element_type=jnp.float32))
    layer_out = (after_mix + routed + gate_value[:, None] * shared).astype(jnp.bfloat16)
    return (layer_out, new_state)
```

```python
import jax
import jax.numpy as jnp
from jax import lax
from jax.sharding import PartitionSpec as P

norm_eps = 1e-05
routed_scale = 2.5
f32 = jnp.float32
bf16 = jnp.bfloat16
cores = 2


def y_shift(tp_count, step):
    chips = tp_count // cores
    return [
        (y * cores + c, ((y + step) % chips) * cores + c)
        for y in range(chips)
        for c in range(cores)
    ]


def core_swap(tp_count):
    return [(i, i ^ 1) for i in range(tp_count)]


def hop_gather(array, tp_count):
    chips = tp_count // cores
    parts = [array] + [
        lax.ppermute(array, "tp", y_shift(tp_count, step)) for step in range(1, chips)
    ]
    mine = jnp.stack(parts)
    other = lax.ppermute(mine, "tp", core_swap(tp_count))
    return mine, other


def natural_blocks(mine, other, tp_count, place):
    chips = tp_count // cores
    y, c = place // cores, place % cores
    even = jnp.where(c == 0, mine, other)
    odd = jnp.where(c == 0, other, mine)
    blocks = []
    for b in range(tp_count):
        k = (y - b // cores) % chips
        blocks.append(lax.dynamic_index_in_dim(even if b % cores == 0 else odd, k, 0, False))
    return jnp.concatenate(blocks, axis=1)


def layer_norm(values, gain_vec):
    row_mean = jnp.mean(values, axis=-1, keepdims=True)
    row_square = jnp.mean(values * values, axis=-1, keepdims=True)
    return (values - row_mean) * lax.rsqrt(row_square - row_mean * row_mean + norm_eps) * gain_vec


def coefficients(decay_rate, frequency, log_step, in_coef):
    time_step = jnp.exp(log_step)[:, None]
    real_rate = -decay_rate
    magnitude = jnp.exp(real_rate * time_step)
    keep_re = magnitude * jnp.cos(frequency * time_step)
    keep_im = magnitude * jnp.sin(frequency * time_step)
    denominator = real_rate * real_rate + frequency * frequency
    factor_re = ((keep_re - 1.0) * real_rate + keep_im * frequency) / denominator
    factor_im = (keep_im * real_rate - (keep_re - 1.0) * frequency) / denominator
    push_re = factor_re[..., None] * in_coef[0] - factor_im[..., None] * in_coef[1]
    push_im = factor_re[..., None] * in_coef[1] + factor_im[..., None] * in_coef[0]
    return (keep_re, keep_im, push_re, push_im)


def mixer_step(
    normed, in_weight, state, decay_rate, frequency, log_step, in_coef, out_coef, skip_gain
):
    row_count = normed.shape[0]
    group_count, state_count = decay_rate.shape
    keep_re, keep_im, push_re, push_im = coefficients(decay_rate, frequency, log_step, in_coef)
    drive = jnp.dot(normed, in_weight, preferred_element_type=f32).astype(bf16)
    drive_f = drive.astype(f32).reshape(row_count, group_count, -1)
    input_re = jnp.einsum("tgh,gph->tgp", drive_f, push_re)
    input_im = jnp.einsum("tgh,gph->tgp", drive_f, push_im)
    old_re = state[0].reshape(row_count, group_count, state_count)
    old_im = state[1].reshape(row_count, group_count, state_count)
    new_re = keep_re * old_re - keep_im * old_im + input_re
    new_im = keep_re * old_im + keep_im * old_re + input_im
    read_out = jnp.einsum("ghp,tgp->tgh", out_coef[0], new_re) - jnp.einsum(
        "ghp,tgp->tgh", out_coef[1], new_im
    )
    read_out = read_out.reshape(row_count, -1) + skip_gain * drive_f.reshape(row_count, -1)
    mixed_rows = jax.nn.gelu(read_out, approximate=True).astype(bf16)
    updated = jnp.stack([new_re.reshape(row_count, -1), new_im.reshape(row_count, -1)])
    return (mixed_rows, updated)


def slot_tables(routes, route_weight, place, tp_count, ep_count, capacity):
    rows, top = routes.shape
    slots = ep_count * capacity
    slot = lax.broadcasted_iota(jnp.int32, (rows, slots), 1)
    expert_of = (slot // capacity) * tp_count + place
    hits = [routes[:, j : j + 1] == expert_of for j in range(top)]
    named = hits[0]
    for h in hits[1:]:
        named = named | h
    i = lax.broadcasted_iota(jnp.int32, (rows, rows), 0)
    j = lax.broadcasted_iota(jnp.int32, (rows, rows), 1)
    rank = jnp.dot(
        (j < i).astype(bf16), named.astype(bf16), preferred_element_type=f32
    ).astype(jnp.int32)
    picked = named & (rank == slot % capacity)
    weights = route_weight / jnp.sum(route_weight, axis=-1, keepdims=True) * routed_scale
    share = sum(jnp.where(h, weights[:, n : n + 1], 0.0) for n, h in enumerate(hits))
    share = jnp.where(picked, share, 0.0)
    return picked.astype(bf16), share


def per_device(
    residual,
    in_gain,
    in_weight,
    state,
    decay_rate,
    frequency,
    log_step,
    in_coef,
    out_coef,
    skip_gain,
    out_weight,
    mid_gain,
    gate_vector,
    routes,
    route_weight,
    expert_gate,
    expert_up,
    expert_down,
    shared_gate,
    shared_up,
    shared_down,
):
    tp_count = lax.axis_size("tp")
    ep_count = lax.axis_size("ep")
    chips = tp_count // cores
    place = lax.axis_index("tp")
    seq_rows, feat_part = residual.shape
    width = feat_part * tp_count
    per_dev = seq_rows // tp_count
    capacity = max(2, 2 * seq_rows * routes.shape[1] // (ep_count * tp_count))
    slots = ep_count * capacity

    full_resid = natural_blocks(*hop_gather(residual, tp_count), tp_count, place).astype(f32)
    normed = layer_norm(full_resid, in_gain).astype(bf16)
    mixed_part, new_state = mixer_step(
        normed, in_weight, state, decay_rate, frequency, log_step, in_coef, out_coef, skip_gain
    )
    mixed_rows = natural_blocks(*hop_gather(mixed_part, tp_count), tp_count, place)
    after_mix = full_resid + jnp.dot(mixed_rows, out_weight, preferred_element_type=f32)
    normed_mid = layer_norm(after_mix, mid_gain).astype(bf16)
    own_mid = lax.dynamic_slice_in_dim(normed_mid, place * per_dev, per_dev, 0)
    own_after = lax.dynamic_slice_in_dim(after_mix, place * per_dev, per_dev, 0)

    picked, share = slot_tables(routes, route_weight, place, tp_count, ep_count, capacity)
    outgoing = lax.dot_general(
        picked, normed_mid, (((0,), (0,)), ((), ())), preferred_element_type=f32
    ).astype(bf16)
    outgoing = outgoing.reshape(ep_count, capacity, width)
    copies = jnp.broadcast_to(own_mid[None], (ep_count, per_dev, width))
    got = lax.all_to_all(
        jnp.concatenate([outgoing, copies], axis=1), "ep", split_axis=0, concat_axis=0, tiled=True
    )
    slot_rows = got[:, :capacity].reshape(slots, width)
    piece = got[:, capacity:].reshape(ep_count * per_dev, width)

    gate_part = jnp.dot(slot_rows, expert_gate[0], preferred_element_type=f32)
    up_part = jnp.dot(slot_rows, expert_up[0], preferred_element_type=f32)
    hidden = (jax.nn.silu(gate_part) * up_part).astype(bf16)
    result = jnp.dot(hidden, expert_down[0], preferred_element_type=f32).astype(bf16)
    returned = lax.all_to_all(
        result.reshape(ep_count, capacity, width), "ep", split_axis=0, concat_axis=0, tiled=True
    ).reshape(slots, width)

    gate_part = jnp.dot(piece, shared_gate, preferred_element_type=f32)
    up_part = jnp.dot(piece, shared_up, preferred_element_type=f32)
    shared_hidden = (jax.nn.silu(gate_part) * up_part).astype(bf16)
    partial_rows = jnp.dot(shared_hidden, shared_down, preferred_element_type=f32).astype(bf16)
    partial_rows, returned = lax.optimization_barrier((partial_rows, returned))
    partial_back = lax.all_to_all(
        partial_rows.reshape(ep_count, per_dev, width), "ep", split_axis=0, concat_axis=0, tiled=True
    )
    shared = jnp.sum(partial_back.astype(f32), axis=0)

    r = jnp.arange(seq_rows, dtype=jnp.int32)
    ahead = (r // per_dev) % chips
    core = (place % cores) ^ (r // (per_dev * chips))
    source = (((place // cores + ahead) % chips) * cores + core) * per_dev + r % per_dev
    turn = (source[:, None] == r[None, :]).astype(bf16)
    share_hi = share.astype(bf16)
    share_lo = (share - share_hi.astype(f32)).astype(bf16)
    share_hi = jnp.dot(turn, share_hi, preferred_element_type=f32).astype(bf16)
    share_lo = jnp.dot(turn, share_lo, preferred_element_type=f32).astype(bf16)
    both = jnp.dot(
        jnp.concatenate([share_hi, share_lo], axis=1),
        jnp.concatenate([returned, returned], axis=0),
        preferred_element_type=f32,
    )
    half = per_dev * chips
    theirs = lax.ppermute(both[half:].astype(bf16), "tp", core_swap(tp_count))
    pair = both[:half] + theirs.astype(f32)
    routed = pair[:per_dev]
    pair = pair.astype(bf16)
    for step in range(1, chips):
        routed = routed + lax.ppermute(
            pair[step * per_dev : (step + 1) * per_dev], "tp", y_shift(tp_count, step)
        ).astype(f32)
    gate_value = jax.nn.sigmoid(jnp.dot(own_mid, gate_vector, preferred_element_type=f32))
    layer_out = (own_after + routed + gate_value[:, None] * shared).astype(bf16)
    return (layer_out, new_state)


def solution(mesh):
    return jax.shard_map(
        per_device,
        mesh=mesh,
        in_specs=(
            P("ep", "tp"),
            P(),
            P(None, "tp"),
            P(None, "ep", "tp"),
            P("tp", None),
            P("tp", None),
            P("tp"),
            P(None, "tp", None, None),
            P(None, "tp", None, None),
            P("tp"),
            P(),
            P(),
            P(),
            P("ep", None),
            P("ep", None),
            P(("ep", "tp"), None, None),
            P(("ep", "tp"), None, None),
            P(("ep", "tp"), None, None),
            P(None, "ep"),
            P(None, "ep"),
            P("ep", None),
        ),
        out_specs=(P(("ep", "tp"), None), P(None, "ep", "tp")),
        check_vma=False,
    )
```

```python
import functools
import math

import jax
import jax.numpy as jnp
from jax import lax
from jax.experimental import pallas as pl
from jax.experimental.pallas import tpu as pltpu
from jax.sharding import PartitionSpec as P


norm_eps = 1e-05
routed_scale = 2.5
f32 = jnp.float32
bf16 = jnp.bfloat16
cores = 2


def y_shift(tp_count, step):
    chips = tp_count // cores
    return [
        (y * cores + c, ((y + step) % chips) * cores + c)
        for y in range(chips)
        for c in range(cores)
    ]


def core_swap(tp_count):
    return [(i, i ^ 1) for i in range(tp_count)]


def hop_gather(array, tp_count):
    chips = tp_count // cores
    mine = [array] + [
        lax.ppermute(array, "tp", y_shift(tp_count, step)) for step in range(1, chips)
    ]
    other = [lax.ppermute(part, "tp", core_swap(tp_count)) for part in mine]
    return mine, other


def plane_shift(ep_count, z_step, x_step):
    side = math.isqrt(ep_count)
    return [
        (z * side + x, ((z + z_step) % side) * side + (x + x_step) % side)
        for z in range(side)
        for x in range(side)
    ]


def natural_blocks(mine, other, tp_count, place):
    chips = tp_count // cores
    y, c = place // cores, place % cores
    even = jnp.where(c == 0, mine, other)
    odd = jnp.where(c == 0, other, mine)
    blocks = []
    for b in range(tp_count):
        k = (y - b // cores) % chips
        blocks.append(lax.dynamic_index_in_dim(even if b % cores == 0 else odd, k, 0, False))
    return jnp.concatenate(blocks, axis=1)


def layer_norm(values, gain_vec):
    row_mean = jnp.mean(values, axis=-1, keepdims=True)
    row_square = jnp.mean(values * values, axis=-1, keepdims=True)
    return (values - row_mean) * lax.rsqrt(row_square - row_mean * row_mean + norm_eps) * gain_vec


def coefficients(decay_rate, frequency, log_step, in_coef):
    time_step = jnp.exp(log_step)[:, None]
    real_rate = -decay_rate
    magnitude = jnp.exp(real_rate * time_step)
    keep_re = magnitude * jnp.cos(frequency * time_step)
    keep_im = magnitude * jnp.sin(frequency * time_step)
    denominator = real_rate * real_rate + frequency * frequency
    factor_re = ((keep_re - 1.0) * real_rate + keep_im * frequency) / denominator
    factor_im = (keep_im * real_rate - (keep_re - 1.0) * frequency) / denominator
    push_re = factor_re[..., None] * in_coef[0] - factor_im[..., None] * in_coef[1]
    push_im = factor_re[..., None] * in_coef[1] + factor_im[..., None] * in_coef[0]
    return (keep_re, keep_im, push_re, push_im)


def mixer_step(
    normed, in_weight, state, decay_rate, frequency, log_step, in_coef, out_coef, skip_gain
):
    row_count = normed.shape[0]
    group_count, state_count = decay_rate.shape
    keep_re, keep_im, push_re, push_im = coefficients(decay_rate, frequency, log_step, in_coef)
    drive = jnp.dot(normed, in_weight, preferred_element_type=f32).astype(bf16)
    drive_f = drive.astype(f32).reshape(row_count, group_count, -1)
    input_re = jnp.einsum("tgh,gph->tgp", drive_f, push_re)
    input_im = jnp.einsum("tgh,gph->tgp", drive_f, push_im)
    old_re = state[0].reshape(row_count, group_count, state_count)
    old_im = state[1].reshape(row_count, group_count, state_count)
    new_re = keep_re * old_re - keep_im * old_im + input_re
    new_im = keep_re * old_im + keep_im * old_re + input_im
    read_out = jnp.einsum("ghp,tgp->tgh", out_coef[0], new_re) - jnp.einsum(
        "ghp,tgp->tgh", out_coef[1], new_im
    )
    read_out = read_out.reshape(row_count, -1) + skip_gain * drive_f.reshape(row_count, -1)
    mixed_rows = jax.nn.gelu(read_out, approximate=True).astype(bf16)
    updated = jnp.stack([new_re.reshape(row_count, -1), new_im.reshape(row_count, -1)])
    return (mixed_rows, updated)


def in_hbm():
    return pl.BlockSpec(memory_space=pltpu.HBM)


def in_vmem():
    return pl.BlockSpec(memory_space=pltpu.VMEM)


def in_smem():
    return pl.BlockSpec(memory_space=pltpu.SMEM)


def mm(a, b):
    return jnp.dot(a, b, preferred_element_type=f32)


def expert_body(
    rows_hbm, gate_hbm, up_hbm, down_hbm, out_hbm, rows, gate, up, down, hidden, out, sems
):
    cuts = gate.shape[0]
    load_rows = pltpu.make_async_copy(rows_hbm, rows, sems.at[0])
    load_rows.start()
    loads = []
    for i in range(cuts):
        pair = (
            pltpu.make_async_copy(gate_hbm.at[i], gate.at[i], sems.at[1 + 2 * i]),
            pltpu.make_async_copy(up_hbm.at[i], up.at[i], sems.at[2 + 2 * i]),
        )
        for copy in pair:
            copy.start()
        loads.append(pair)
    parts = down.shape[0]
    tail = [
        pltpu.make_async_copy(down_hbm.at[i], down.at[i], sems.at[1 + 2 * cuts + i])
        for i in range(parts)
    ]
    for copy in tail:
        copy.start()
    load_rows.wait()
    gate_part = up_part = None
    depth = gate.shape[1]
    for i in range(cuts):
        for copy in loads[i]:
            copy.wait()
        block = rows[:, i * depth : (i + 1) * depth]
        g, u = mm(block, gate[i]), mm(block, up[i])
        gate_part = g if gate_part is None else gate_part + g
        up_part = u if up_part is None else up_part + u
    hidden[...] = (gate_part * jax.nn.sigmoid(gate_part) * up_part).astype(bf16)
    total = None
    depth = down.shape[1]
    for i in range(parts):
        tail[i].wait()
        piece = mm(hidden[:, i * depth : (i + 1) * depth], down[i])
        total = piece if total is None else total + piece
    out[...] = total.astype(bf16)
    store = pltpu.make_async_copy(out, out_hbm, sems.at[0])
    store.start()
    store.wait()


def expert_kernel(rows, gate, up, down):
    count, width = rows.shape
    inner = gate.shape[1]
    cuts, parts = 4, 2
    return pl.pallas_call(
        expert_body,
        out_shape=jax.ShapeDtypeStruct((count, width), bf16),
        in_specs=[in_hbm()] * 4,
        out_specs=in_hbm(),
        scratch_shapes=[
            pltpu.VMEM((count, width), bf16),
            pltpu.VMEM((cuts, width // cuts, inner), bf16),
            pltpu.VMEM((cuts, width // cuts, inner), bf16),
            pltpu.VMEM((parts, inner // parts, width), bf16),
            pltpu.VMEM((count, inner), bf16),
            pltpu.VMEM((count, width), bf16),
            pltpu.SemaphoreType.DMA((1 + 2 * cuts + parts,)),
        ],
        compiler_params=pltpu.CompilerParams(vmem_limit_bytes=60 * 1024 * 1024),
        name="expert_mlp",
    )(
        rows,
        gate.reshape(cuts, width // cuts, inner),
        up.reshape(cuts, width // cuts, inner),
        down.reshape(parts, inner // parts, width),
    )


def shared_body(place, *refs, side):
    planes, refs = refs[:side], refs[side:]
    z, x = lax.div(place[0], side), lax.rem(place[0], side)
    order = [
        lax.rem(z + side - i, side) * side + lax.rem(x + side - j, side)
        for i in range(side)
        for j in range(side)
    ]
    gate_hbm, up_hbm, down_hbm, out_hbm, gate, up, down, rows, out, sems = refs
    loads = [
        pltpu.make_async_copy(gate_hbm, gate, sems.at[0]),
        pltpu.make_async_copy(up_hbm, up, sems.at[1]),
        pltpu.make_async_copy(down_hbm, down, sems.at[2]),
    ]
    moves = [
        pltpu.make_async_copy(plane, rows.at[i], sems.at[3 + i]) for i, plane in enumerate(planes)
    ]
    for copy in moves + loads:
        copy.start()
    for copy in moves + loads[:2]:
        copy.wait()
    per = rows.shape[1] // side
    for half in range(2):
        x = rows[half * 2 : half * 2 + 2].reshape(2 * rows.shape[1], rows.shape[2])
        gate_part = mm(x, gate[...])
        up_part = mm(x, up[...])
        hidden = (gate_part * jax.nn.sigmoid(gate_part) * up_part).astype(bf16)
        if half == 0:
            loads[2].wait()
        result = mm(hidden, down[...]).astype(bf16)
        for k in range(2 * side):
            block = order[half * 2 * side + k]
            out[pl.ds(pl.multiple_of(block * per, per), per), :] = result[k * per : (k + 1) * per]
    store = pltpu.make_async_copy(out, out_hbm, sems.at[0])
    store.start()
    store.wait()


def shared_kernel(place, planes, gate, up, down):
    count, width = planes[0].shape
    inner = gate.shape[1]
    side = len(planes)
    return pl.pallas_call(
        functools.partial(shared_body, side=side),
        out_shape=jax.ShapeDtypeStruct((count * side, width), bf16),
        in_specs=[in_smem()] + [in_hbm()] * (side + 3),
        out_specs=in_hbm(),
        scratch_shapes=[
            pltpu.VMEM((width, inner), bf16),
            pltpu.VMEM((width, inner), bf16),
            pltpu.VMEM((inner, width), bf16),
            pltpu.VMEM((side, count, width), bf16),
            pltpu.VMEM((count * side, width), bf16),
            pltpu.SemaphoreType.DMA((3 + side,)),
        ],
        compiler_params=pltpu.CompilerParams(vmem_limit_bytes=60 * 1024 * 1024),
        name="shared_mlp",
    )(place, *planes, gate, up, down)


def mid_body(place, *refs, tp):
    resid, mixed, refs = refs[:tp], refs[tp : 2 * tp], refs[2 * tp :]
    chips = tp // cores
    chip, core = lax.div(place[0], cores), lax.rem(place[0], cores)
    order = [
        lax.rem(chip + chips - k, chips) * cores + (core ^ other)
        for other in range(cores)
        for k in range(chips)
    ]
    weight_hbm, gain, picked, own_mid, after_hbm, outgoing_hbm, weight, rows, total, normed, outgoing, sems = refs
    cuts = weight.shape[0]
    loads = [
        pltpu.make_async_copy(weight_hbm.at[i], weight.at[i], sems.at[i]) for i in range(cuts)
    ]
    for copy in loads:
        copy.start()
    feat, chan = resid[0].shape[1], mixed[0].shape[1]
    for i in range(tp):
        at = pl.multiple_of(order[i] * feat, feat)
        total[:, pl.ds(at, feat)] = resid[i][...].astype(f32)
        at = pl.multiple_of(order[i] * chan, chan)
        rows[:, pl.ds(at, chan)] = mixed[i][...]
    depth = weight.shape[1]
    for i in range(cuts):
        loads[i].wait()
        total[...] += mm(rows[:, i * depth : (i + 1) * depth], weight[i])
    values = total[...]
    mean = jnp.mean(values, axis=-1, keepdims=True)
    square = jnp.mean(values * values, axis=-1, keepdims=True)
    scale = lax.rsqrt(square - mean * mean + norm_eps)
    normed[...] = ((values - mean) * scale * gain[...]).astype(bf16)
    per = own_mid.shape[0]
    at = pl.multiple_of(place[0] * per, per)
    own_mid[...] = normed[pl.ds(at, per), :]
    keep = pltpu.make_async_copy(total.at[pl.ds(at, per), :], after_hbm, sems.at[0])
    keep.start()
    outgoing[...] = mm(picked[...], normed[...]).astype(bf16)
    store = pltpu.make_async_copy(outgoing, outgoing_hbm, sems.at[1])
    store.start()
    keep.wait()
    store.wait()


def mid_kernel(place, resid, mixed, weight, gain, picked):
    tp = len(resid)
    rows, feat = resid[0].shape
    chan = mixed[0].shape[1]
    width = feat * tp
    cuts = 8
    per = rows // tp
    return pl.pallas_call(
        functools.partial(mid_body, tp=tp),
        out_shape=(
            jax.ShapeDtypeStruct((per, width), bf16),
            jax.ShapeDtypeStruct((per, width), f32),
            jax.ShapeDtypeStruct((picked.shape[0], width), bf16),
        ),
        in_specs=[in_smem()] + [in_vmem()] * (2 * tp) + [in_hbm()] + [in_vmem()] * 2,
        out_specs=(in_vmem(), in_hbm(), in_hbm()),
        scratch_shapes=[
            pltpu.VMEM((cuts, chan * tp // cuts, width), bf16),
            pltpu.VMEM((rows, chan * tp), bf16),
            pltpu.VMEM((rows, width), f32),
            pltpu.VMEM((rows, width), bf16),
            pltpu.VMEM((picked.shape[0], width), bf16),
            pltpu.SemaphoreType.DMA((cuts,)),
        ],
        compiler_params=pltpu.CompilerParams(vmem_limit_bytes=60 * 1024 * 1024),
        name="out_proj_norm",
    )(
        place,
        *resid,
        *mixed,
        weight.reshape(cuts, chan * tp // cuts, width),
        gain.reshape(1, width),
        picked,
    )


def join_body(*refs):
    parts, out, sems = refs[:-2], refs[-2], refs[-1]
    per = parts[0].shape[0]
    moves = [
        pltpu.make_async_copy(part, out.at[pl.ds(i * per, per), :], sems.at[i])
        for i, part in enumerate(parts)
    ]
    for copy in moves:
        copy.start()
    for copy in moves:
        copy.wait()


def join_kernel(parts):
    per, width = parts[0].shape
    return pl.pallas_call(
        join_body,
        out_shape=jax.ShapeDtypeStruct((per * len(parts), width), parts[0].dtype),
        in_specs=[in_vmem()] * len(parts),
        out_specs=in_hbm(),
        scratch_shapes=[pltpu.SemaphoreType.DMA((len(parts),))],
        compiler_params=pltpu.CompilerParams(vmem_limit_bytes=60 * 1024 * 1024),
        name="join_rows",
    )(*parts)


def tables_body(place, routes, weights, picked_out, share_out, *, experts, tp_count):
    top, rows = routes.shape
    slots = picked_out.shape[0]
    capacity = slots * tp_count // experts
    tp = place[0]
    chips = tp_count // cores
    per = rows // tp_count
    slot = lax.broadcasted_iota(jnp.int32, (slots, rows), 0)
    wanted = (slot // capacity) * tp_count + tp
    total = jnp.sum(weights[...], axis=0, keepdims=True)
    named = routes[0:1, :] == wanted
    share = jnp.where(named, weights[0:1, :] / total * routed_scale, 0.0)
    for j in range(1, top):
        hit = routes[j : j + 1, :] == wanted
        named = named | hit
        share = share + jnp.where(hit, weights[j : j + 1, :] / total * routed_scale, 0.0)
    down = lax.broadcasted_iota(jnp.int32, (rows, rows), 0)
    across = lax.broadcasted_iota(jnp.int32, (rows, rows), 1)
    rank = mm(named.astype(f32).astype(bf16), (down < across).astype(f32).astype(bf16))
    picked = named & (rank == (slot % capacity).astype(f32))
    picked_out[...] = jnp.where(picked, 1.0, 0.0).astype(bf16)
    share = jnp.where(picked, share, 0.0)
    high = share.astype(bf16)
    low = (share - high.astype(f32)).astype(bf16)
    ahead = (across // per) % chips
    core = (tp % cores) ^ (across // (per * chips))
    source = (((tp // cores + ahead) % chips) * cores + core) * per + across % per
    turn = (source == down).astype(f32).astype(bf16)
    share_out[:slots, :] = mm(high, turn).astype(bf16)
    share_out[slots:, :] = mm(low, turn).astype(bf16)


def tables_kernel(place, routes, weights, experts, tp_count):
    rows, top = routes.shape
    slots = max(2, 2 * rows * top // experts) * (experts // tp_count)
    return pl.pallas_call(
        functools.partial(tables_body, experts=experts, tp_count=tp_count),
        out_shape=(
            jax.ShapeDtypeStruct((slots, rows), bf16),
            jax.ShapeDtypeStruct((2 * slots, rows), bf16),
        ),
        in_specs=[in_smem()] + [in_vmem()] * 2,
        out_specs=(in_vmem(),) * 2,
        compiler_params=pltpu.CompilerParams(vmem_limit_bytes=60 * 1024 * 1024),
        name="slot_tables",
    )(place, routes.T, weights.T)


def layer(
    residual,
    in_gain,
    in_weight,
    state,
    decay_rate,
    frequency,
    log_step,
    in_coef,
    out_coef,
    skip_gain,
    out_weight,
    mid_gain,
    gate_vector,
    routes,
    route_weight,
    expert_gate,
    expert_up,
    expert_down,
    shared_gate,
    shared_up,
    shared_down,
):
    tp_count = lax.axis_size("tp")
    ep_count = lax.axis_size("ep")
    chips = tp_count // cores
    place = lax.axis_index("tp")
    seq_rows, feat_part = residual.shape
    width = feat_part * tp_count
    per_dev = seq_rows // tp_count
    capacity = max(2, 2 * seq_rows * routes.shape[1] // (ep_count * tp_count))
    slots = ep_count * capacity

    resid_mine, resid_other = hop_gather(residual, tp_count)
    full_resid = natural_blocks(jnp.stack(resid_mine), jnp.stack(resid_other), tp_count, place).astype(f32)
    normed = layer_norm(full_resid, in_gain).astype(bf16)
    mixed_part, new_state = mixer_step(
        normed, in_weight, state, decay_rate, frequency, log_step, in_coef, out_coef, skip_gain
    )
    picked, share = tables_kernel(
        place.reshape(1), routes, route_weight, ep_count * tp_count, tp_count
    )
    mixed_mine, mixed_other = hop_gather(mixed_part, tp_count)
    own_mid, own_after, outgoing = mid_kernel(
        place.reshape(1), resid_mine + resid_other, mixed_mine + mixed_other, out_weight, mid_gain, picked
    )

    side = math.isqrt(ep_count)
    line = [own_mid] + [
        lax.ppermute(own_mid, "ep", plane_shift(ep_count, 0, step)) for step in range(1, side)
    ]
    line = join_kernel(line)
    plane = [line] + [
        lax.ppermute(line, "ep", plane_shift(ep_count, step, 0)) for step in range(1, side)
    ]
    slot_rows = lax.all_to_all(
        outgoing.reshape(ep_count, capacity, width), "ep", split_axis=0, concat_axis=0, tiled=True
    ).reshape(slots, width)

    result = expert_kernel(slot_rows, expert_gate[0], expert_up[0], expert_down[0])
    returned = lax.all_to_all(
        result.reshape(ep_count, capacity, width), "ep", split_axis=0, concat_axis=0, tiled=True
    ).reshape(slots, width)

    partial_rows = shared_kernel(lax.axis_index("ep").reshape(1), plane, shared_gate, shared_up, shared_down)
    partial_back = lax.all_to_all(
        partial_rows.reshape(ep_count, per_dev, width), "ep", split_axis=0, concat_axis=0, tiled=True
    )
    shared = jnp.sum(partial_back.astype(f32), axis=0)

    both = lax.dot_general(
        share,
        jnp.concatenate([returned, returned], axis=0),
        (((0,), (0,)), ((), ())),
        preferred_element_type=f32,
    )
    half = per_dev * chips
    theirs = lax.ppermute(both[half:].astype(bf16), "tp", core_swap(tp_count))
    pair = both[:half] + theirs.astype(f32)
    routed = pair[:per_dev]
    pair = pair.astype(bf16)
    for step in range(1, chips):
        routed = routed + lax.ppermute(
            pair[step * per_dev : (step + 1) * per_dev], "tp", y_shift(tp_count, step)
        ).astype(f32)
    gate_value = jax.nn.sigmoid(jnp.dot(own_mid, gate_vector, preferred_element_type=f32))
    layer_out = (own_after + routed + gate_value[:, None] * shared).astype(bf16)
    return (layer_out, new_state)


def solution(mesh):
    return jax.shard_map(
        layer,
        mesh=mesh,
        in_specs=(
            P("ep", "tp"),
            P(),
            P(None, "tp"),
            P(None, "ep", "tp"),
            P("tp", None),
            P("tp", None),
            P("tp"),
            P(None, "tp", None, None),
            P(None, "tp", None, None),
            P("tp"),
            P(),
            P(),
            P(),
            P("ep", None),
            P("ep", None),
            P(("ep", "tp"), None, None),
            P(("ep", "tp"), None, None),
            P(("ep", "tp"), None, None),
            P(None, "ep"),
            P(None, "ep"),
            P("ep", None),
        ),
        out_specs=(P(("ep", "tp"), None), P(None, "ep", "tp")),
        check_vma=False,
    )
```

```python
import functools
import math

import jax
import jax.numpy as jnp
from jax import lax
from jax.experimental import pallas as pl
from jax.experimental.pallas import tpu as pltpu
from jax.sharding import PartitionSpec as P


norm_eps = 1e-05
routed_scale = 2.5
f32 = jnp.float32
bf16 = jnp.bfloat16
cores = 2


def y_shift(tp_count, step):
    chips = tp_count // cores
    return [
        (y * cores + c, ((y + step) % chips) * cores + c)
        for y in range(chips)
        for c in range(cores)
    ]


def core_swap(tp_count):
    return [(i, i ^ 1) for i in range(tp_count)]


def hop_gather(array, tp_count):
    chips = tp_count // cores
    mine = [array] + [
        lax.ppermute(array, "tp", y_shift(tp_count, step)) for step in range(1, chips)
    ]
    other = [lax.ppermute(part, "tp", core_swap(tp_count)) for part in mine]
    return mine, other


def plane_shift(ep_count, z_step, x_step):
    side = math.isqrt(ep_count)
    return [
        (z * side + x, ((z + z_step) % side) * side + (x + x_step) % side)
        for z in range(side)
        for x in range(side)
    ]


def weight_moves(ep_count, tp_count, core):
    side = math.isqrt(ep_count)
    moves = []
    for e in range(ep_count):
        far = (side - 1 - e // side) * side + e % side
        for t in range(tp_count):
            to = far if t % cores == core else e
            moves.append((e * tp_count + t, to * tp_count + (t ^ 1)))
    return moves


def pair_swap(ep_count):
    side = math.isqrt(ep_count)
    return [(e, ((e // side) ^ 1) * side + e % side) for e in range(ep_count)]


def natural_blocks(mine, other, tp_count, place):
    chips = tp_count // cores
    y, c = place // cores, place % cores
    even = jnp.where(c == 0, mine, other)
    odd = jnp.where(c == 0, other, mine)
    blocks = []
    for b in range(tp_count):
        k = (y - b // cores) % chips
        blocks.append(lax.dynamic_index_in_dim(even if b % cores == 0 else odd, k, 0, False))
    return jnp.concatenate(blocks, axis=1)


def layer_norm(values, gain_vec):
    row_mean = jnp.mean(values, axis=-1, keepdims=True)
    row_square = jnp.mean(values * values, axis=-1, keepdims=True)
    return (values - row_mean) * lax.rsqrt(row_square - row_mean * row_mean + norm_eps) * gain_vec


def coefficients(decay_rate, frequency, log_step, in_coef):
    time_step = jnp.exp(log_step)[:, None]
    real_rate = -decay_rate
    magnitude = jnp.exp(real_rate * time_step)
    keep_re = magnitude * jnp.cos(frequency * time_step)
    keep_im = magnitude * jnp.sin(frequency * time_step)
    denominator = real_rate * real_rate + frequency * frequency
    factor_re = ((keep_re - 1.0) * real_rate + keep_im * frequency) / denominator
    factor_im = (keep_im * real_rate - (keep_re - 1.0) * frequency) / denominator
    push_re = factor_re[..., None] * in_coef[0] - factor_im[..., None] * in_coef[1]
    push_im = factor_re[..., None] * in_coef[1] + factor_im[..., None] * in_coef[0]
    return (keep_re, keep_im, push_re, push_im)


def mixer_step(
    normed, in_weight, state, decay_rate, frequency, log_step, in_coef, out_coef, skip_gain
):
    row_count = normed.shape[0]
    group_count, state_count = decay_rate.shape
    keep_re, keep_im, push_re, push_im = coefficients(decay_rate, frequency, log_step, in_coef)
    drive = jnp.dot(normed, in_weight, preferred_element_type=f32).astype(bf16)
    drive_f = drive.astype(f32).reshape(row_count, group_count, -1)
    input_re = jnp.einsum("tgh,gph->tgp", drive_f, push_re)
    input_im = jnp.einsum("tgh,gph->tgp", drive_f, push_im)
    old_re = state[0].reshape(row_count, group_count, state_count)
    old_im = state[1].reshape(row_count, group_count, state_count)
    new_re = keep_re * old_re - keep_im * old_im + input_re
    new_im = keep_re * old_im + keep_im * old_re + input_im
    read_out = jnp.einsum("ghp,tgp->tgh", out_coef[0], new_re) - jnp.einsum(
        "ghp,tgp->tgh", out_coef[1], new_im
    )
    read_out = read_out.reshape(row_count, -1) + skip_gain * drive_f.reshape(row_count, -1)
    mixed_rows = jax.nn.gelu(read_out, approximate=True).astype(bf16)
    updated = jnp.stack([new_re.reshape(row_count, -1), new_im.reshape(row_count, -1)])
    return (mixed_rows, updated)


def in_hbm():
    return pl.BlockSpec(memory_space=pltpu.HBM)


def in_vmem():
    return pl.BlockSpec(memory_space=pltpu.VMEM)


def in_smem():
    return pl.BlockSpec(memory_space=pltpu.SMEM)


def mm(a, b):
    return jnp.dot(a, b, preferred_element_type=f32)


def expert_body(
    rows_hbm, gate_hbm, up_hbm, down_hbm, out_hbm, rows, gate, up, down, hidden, out, sems
):
    cuts, depth = gate.shape[0], gate.shape[1]
    halves = down.shape[0]
    load_rows = pltpu.make_async_copy(rows_hbm, rows, sems.at[0])
    load_rows.start()
    loads = []
    for i in range(cuts):
        pair = (
            pltpu.make_async_copy(gate_hbm.at[i], gate.at[i], sems.at[1 + 2 * i]),
            pltpu.make_async_copy(up_hbm.at[i], up.at[i], sems.at[2 + 2 * i]),
        )
        for copy in pair:
            copy.start()
        loads.append(pair)
    span = down.shape[2]
    tail = [
        pltpu.make_async_copy(
            down_hbm.at[:, i * span : (i + 1) * span], down.at[i], sems.at[1 + 2 * cuts + i]
        )
        for i in range(halves)
    ]
    for copy in tail:
        copy.start()
    load_rows.wait()
    gate_part = up_part = None
    for i in range(cuts):
        for copy in loads[i]:
            copy.wait()
        block = rows[:, i * depth : (i + 1) * depth]
        g, u = mm(block, gate[i]), mm(block, up[i])
        gate_part = g if gate_part is None else gate_part + g
        up_part = u if up_part is None else up_part + u
    hidden[...] = (gate_part * jax.nn.sigmoid(gate_part) * up_part).astype(bf16)
    stores = []
    for i in range(halves):
        tail[i].wait()
        out[i] = mm(hidden[...], down[i]).astype(bf16)
        store = pltpu.make_async_copy(
            out.at[i], out_hbm.at[:, i * span : (i + 1) * span], sems.at[1 + 2 * i]
        )
        store.start()
        stores.append(store)
    for store in stores:
        store.wait()


def expert_kernel(rows, gate, up, down):
    count, width = rows.shape
    inner = gate.shape[1]
    cuts, parts = 8, 2
    return pl.pallas_call(
        expert_body,
        out_shape=jax.ShapeDtypeStruct((count, width), bf16),
        in_specs=[in_hbm()] * 4,
        out_specs=in_hbm(),
        scratch_shapes=[
            pltpu.VMEM((count, width), bf16),
            pltpu.VMEM((cuts, width // cuts, inner), bf16),
            pltpu.VMEM((cuts, width // cuts, inner), bf16),
            pltpu.VMEM((parts, inner, width // parts), bf16),
            pltpu.VMEM((count, inner), bf16),
            pltpu.VMEM((parts, count, width // parts), bf16),
            pltpu.SemaphoreType.DMA((1 + 2 * cuts + parts,)),
        ],
        compiler_params=pltpu.CompilerParams(vmem_limit_bytes=60 * 1024 * 1024),
        name="expert_mlp",
    )(
        rows,
        gate.reshape(cuts, width // cuts, inner),
        up.reshape(cuts, width // cuts, inner),
        down,
    )


def shared_body(
    place,
    line_hbm,
    pair_hbm,
    gate_hbm,
    up_hbm,
    down_hbm,
    gate_far,
    up_far,
    down_far,
    gate_swap,
    up_swap,
    down_swap,
    out_hbm,
    gate,
    up,
    down,
    rows,
    out,
    sems,
    *,
    side,
):
    here, core = place[0], lax.rem(place[1], cores)
    z, x = lax.rem(lax.div(here, side), 2), lax.rem(here, side)
    order = [
        lax.rem(z + i, 2) * side + lax.rem(x + side - j, side) for i in range(2) for j in range(side)
    ]
    moves = [
        pltpu.make_async_copy(line_hbm, rows.at[0], sems.at[0]),
        pltpu.make_async_copy(pair_hbm, rows.at[1], sems.at[1]),
    ]
    near = [
        pltpu.make_async_copy(source, target.at[0], sems.at[2 + i])
        for i, (source, target) in enumerate(((gate_hbm, gate), (up_hbm, up), (down_hbm, down)))
    ]
    for copy in moves + near:
        copy.start()

    @pl.when(core == 0)
    def _():
        pltpu.make_async_copy(gate_swap, gate.at[1], sems.at[5]).start()
        pltpu.make_async_copy(up_far, up.at[1], sems.at[6]).start()
        pltpu.make_async_copy(down_swap, down.at[1], sems.at[7]).start()

    @pl.when(core != 0)
    def _():
        pltpu.make_async_copy(gate_far, gate.at[1], sems.at[5]).start()
        pltpu.make_async_copy(up_swap, up.at[1], sems.at[6]).start()
        pltpu.make_async_copy(down_far, down.at[1], sems.at[7]).start()

    far = [
        pltpu.make_async_copy(gate_far, gate.at[1], sems.at[5]),
        pltpu.make_async_copy(up_far, up.at[1], sems.at[6]),
        pltpu.make_async_copy(down_far, down.at[1], sems.at[7]),
    ]
    for copy in moves:
        copy.wait()
    count = 2 * rows.shape[1]
    x_all = rows[...].reshape(count, rows.shape[2])
    hidden = []
    for i, loads in enumerate((near, far)):
        loads[0].wait()
        gate_part = mm(x_all, gate[i])
        loads[1].wait()
        up_part = mm(x_all, up[i])
        hidden.append((gate_part * jax.nn.sigmoid(gate_part) * up_part).astype(bf16))
    near[2].wait()
    far[2].wait()
    per = rows.shape[1] // side
    stores = []
    for half in range(2):
        lo = half * count // 2
        part = slice(lo, lo + count // 2)
        total = mm(hidden[0][part], down[0]) + mm(hidden[1][part], down[1])
        out[part, :] = total.astype(bf16)
        for k in range(half * side, (half + 1) * side):
            at = pl.multiple_of(order[k] * per, per)
            stores.append(
                pltpu.make_async_copy(
                    out.at[k * per : (k + 1) * per, :], out_hbm.at[pl.ds(at, per), :], sems.at[8 + k]
                )
            )
            stores[-1].start()
    for store in stores:
        store.wait()


def shared_kernel(place, line, pair, own, far, swap, side):
    count, width = line.shape
    inner = own[0].shape[1]
    return pl.pallas_call(
        functools.partial(shared_body, side=side),
        out_shape=jax.ShapeDtypeStruct((count * 2, width), bf16),
        in_specs=[in_smem()] + [in_hbm()] * 11,
        out_specs=in_hbm(),
        scratch_shapes=[
            pltpu.VMEM((2, width, inner), bf16),
            pltpu.VMEM((2, width, inner), bf16),
            pltpu.VMEM((2, inner, width), bf16),
            pltpu.VMEM((2, count, width), bf16),
            pltpu.VMEM((count * 2, width), bf16),
            pltpu.SemaphoreType.DMA((8 + 2 * side,)),
        ],
        compiler_params=pltpu.CompilerParams(vmem_limit_bytes=60 * 1024 * 1024),
        name="shared_mlp",
    )(place, line, pair, *own, *far, *swap)


def pull_body(weight_hbm, out, sem):
    copy = pltpu.make_async_copy(weight_hbm, out, sem)
    copy.start()
    copy.wait()


def pull_kernel(weight):
    return pl.pallas_call(
        pull_body,
        out_shape=jax.ShapeDtypeStruct(weight.shape, weight.dtype),
        in_specs=[in_hbm()],
        out_specs=in_vmem(),
        scratch_shapes=[pltpu.SemaphoreType.DMA(())],
        compiler_params=pltpu.CompilerParams(vmem_limit_bytes=8 << 20),
        name="pull_weight",
    )(weight)


def mid_body(place, *refs, tp):
    resid, mixed, refs = refs[:tp], refs[tp : 2 * tp], refs[2 * tp :]
    chips = tp // cores
    chip, core = lax.div(place[0], cores), lax.rem(place[0], cores)
    order = [
        lax.rem(chip + chips - k, chips) * cores + (core ^ other)
        for other in range(cores)
        for k in range(chips)
    ]
    weight, gain, picked, own_mid, after_hbm, outgoing_hbm, rows, total, normed, outgoing, sems = refs
    feat, chan = resid[0].shape[1], mixed[0].shape[1]
    for i in range(tp):
        at = pl.multiple_of(order[i] * feat, feat)
        total[:, pl.ds(at, feat)] = resid[i][...].astype(f32)
        at = pl.multiple_of(order[i] * chan, chan)
        rows[:, pl.ds(at, chan)] = mixed[i][...]
    total[...] += mm(rows[...], weight[...])
    values = total[...]
    mean = jnp.mean(values, axis=-1, keepdims=True)
    square = jnp.mean(values * values, axis=-1, keepdims=True)
    scale = lax.rsqrt(square - mean * mean + norm_eps)
    normed[...] = ((values - mean) * scale * gain[...]).astype(bf16)
    per = own_mid.shape[0]
    at = pl.multiple_of(place[0] * per, per)
    own_mid[...] = normed[pl.ds(at, per), :]
    keep = pltpu.make_async_copy(total.at[pl.ds(at, per), :], after_hbm, sems.at[0])
    keep.start()
    outgoing[...] = mm(picked[...], normed[...]).astype(bf16)
    store = pltpu.make_async_copy(outgoing, outgoing_hbm, sems.at[1])
    store.start()
    keep.wait()
    store.wait()


def mid_kernel(place, resid, mixed, weight, gain, picked):
    tp = len(resid)
    rows, feat = resid[0].shape
    chan = mixed[0].shape[1]
    width = feat * tp
    per = rows // tp
    return pl.pallas_call(
        functools.partial(mid_body, tp=tp),
        out_shape=(
            jax.ShapeDtypeStruct((per, width), bf16),
            jax.ShapeDtypeStruct((per, width), f32),
            jax.ShapeDtypeStruct((picked.shape[0], width), bf16),
        ),
        in_specs=[in_smem()] + [in_vmem()] * (2 * tp + 3),
        out_specs=(in_vmem(), in_hbm(), in_hbm()),
        scratch_shapes=[
            pltpu.VMEM((rows, chan * tp), bf16),
            pltpu.VMEM((rows, width), f32),
            pltpu.VMEM((rows, width), bf16),
            pltpu.VMEM((picked.shape[0], width), bf16),
            pltpu.SemaphoreType.DMA((2,)),
        ],
        compiler_params=pltpu.CompilerParams(vmem_limit_bytes=24 << 20),
        name="out_proj_norm",
    )(
        place,
        *resid,
        *mixed,
        weight,
        gain.reshape(1, width),
        picked,
    )


def join_body(*refs):
    parts, out, sems = refs[:-2], refs[-2], refs[-1]
    per = parts[0].shape[0]
    moves = [
        pltpu.make_async_copy(part, out.at[pl.ds(i * per, per), :], sems.at[i])
        for i, part in enumerate(parts)
    ]
    for copy in moves:
        copy.start()
    for copy in moves:
        copy.wait()


def join_kernel(parts):
    per, width = parts[0].shape
    return pl.pallas_call(
        join_body,
        out_shape=jax.ShapeDtypeStruct((per * len(parts), width), parts[0].dtype),
        in_specs=[in_vmem()] * len(parts),
        out_specs=in_hbm(),
        scratch_shapes=[pltpu.SemaphoreType.DMA((len(parts),))],
        compiler_params=pltpu.CompilerParams(vmem_limit_bytes=8 << 20),
        name="join_rows",
    )(*parts)


def tables_body(place, routes, weights, picked_out, share_out, *, experts, tp_count):
    top, rows = routes.shape
    slots = picked_out.shape[0]
    capacity = slots * tp_count // experts
    tp = place[0]
    chips = tp_count // cores
    per = rows // tp_count
    slot = lax.broadcasted_iota(jnp.int32, (slots, rows), 0)
    wanted = (slot // capacity) * tp_count + tp
    total = jnp.sum(weights[...], axis=0, keepdims=True)
    named = routes[0:1, :] == wanted
    share = jnp.where(named, weights[0:1, :] / total * routed_scale, 0.0)
    for j in range(1, top):
        hit = routes[j : j + 1, :] == wanted
        named = named | hit
        share = share + jnp.where(hit, weights[j : j + 1, :] / total * routed_scale, 0.0)
    down = lax.broadcasted_iota(jnp.int32, (rows, rows), 0)
    across = lax.broadcasted_iota(jnp.int32, (rows, rows), 1)
    rank = mm(named.astype(f32).astype(bf16), (down < across).astype(f32).astype(bf16))
    picked = named & (rank == (slot % capacity).astype(f32))
    picked_out[...] = jnp.where(picked, 1.0, 0.0).astype(bf16)
    share = jnp.where(picked, share, 0.0)
    high = share.astype(bf16)
    low = (share - high.astype(f32)).astype(bf16)
    ahead = (across // per) % chips
    core = (tp % cores) ^ (across // (per * chips))
    source = (((tp // cores + ahead) % chips) * cores + core) * per + across % per
    turn = (source == down).astype(f32).astype(bf16)
    share_out[:slots, :] = mm(high, turn).astype(bf16)
    share_out[slots:, :] = mm(low, turn).astype(bf16)


def tables_kernel(place, routes, weights, experts, tp_count):
    rows, top = routes.shape
    slots = max(2, 2 * rows * top // experts) * (experts // tp_count)
    return pl.pallas_call(
        functools.partial(tables_body, experts=experts, tp_count=tp_count),
        out_shape=(
            jax.ShapeDtypeStruct((slots, rows), bf16),
            jax.ShapeDtypeStruct((2 * slots, rows), bf16),
        ),
        in_specs=[in_smem()] + [in_vmem()] * 2,
        out_specs=(in_vmem(),) * 2,
        compiler_params=pltpu.CompilerParams(vmem_limit_bytes=8 << 20),
        name="slot_tables",
    )(place, routes.T, weights.T)


def layer(
    residual,
    in_gain,
    in_weight,
    state,
    decay_rate,
    frequency,
    log_step,
    in_coef,
    out_coef,
    skip_gain,
    out_weight,
    mid_gain,
    gate_vector,
    routes,
    route_weight,
    expert_gate,
    expert_up,
    expert_down,
    shared_gate,
    shared_up,
    shared_down,
):
    tp_count = lax.axis_size("tp")
    ep_count = lax.axis_size("ep")
    chips = tp_count // cores
    place = lax.axis_index("tp")
    seq_rows, feat_part = residual.shape
    width = feat_part * tp_count
    per_dev = seq_rows // tp_count
    capacity = max(2, 2 * seq_rows * routes.shape[1] // (ep_count * tp_count))
    slots = ep_count * capacity

    resid_mine, resid_other = hop_gather(residual, tp_count)
    own = (shared_gate, shared_up, shared_down)
    far = [
        lax.ppermute(w, ("ep", "tp"), weight_moves(ep_count, tp_count, core))
        for w, core in zip(own, (0, 1, 0))
    ]
    swap = [lax.ppermute(w, "tp", core_swap(tp_count)) for w in far]
    full_resid = natural_blocks(jnp.stack(resid_mine), jnp.stack(resid_other), tp_count, place).astype(f32)
    normed = layer_norm(full_resid, in_gain).astype(bf16)
    mixed_part, new_state = mixer_step(
        normed, in_weight, state, decay_rate, frequency, log_step, in_coef, out_coef, skip_gain
    )
    picked, share = tables_kernel(
        place.reshape(1), routes, route_weight, ep_count * tp_count, tp_count
    )
    mixed_mine, mixed_other = hop_gather(mixed_part, tp_count)
    out_rows = pull_kernel(out_weight)
    own_mid, own_after, outgoing = mid_kernel(
        place.reshape(1), resid_mine + resid_other, mixed_mine + mixed_other, out_rows, mid_gain, picked
    )

    side = math.isqrt(ep_count)
    line = [own_mid]
    for step in range(1, side):
        line.append(lax.ppermute(own_mid, "ep", plane_shift(ep_count, 0, step)))
    line = join_kernel(line)
    pair = lax.ppermute(line, "ep", pair_swap(ep_count))
    slot_rows = lax.all_to_all(
        outgoing.reshape(ep_count, capacity, width), "ep", split_axis=0, concat_axis=0, tiled=True
    ).reshape(slots, width)

    result = expert_kernel(slot_rows, expert_gate[0], expert_up[0], expert_down[0])
    returned = lax.all_to_all(
        result.reshape(ep_count, capacity, width), "ep", split_axis=0, concat_axis=0, tiled=True
    ).reshape(slots, width)

    group = 2 * side
    where = jnp.stack([lax.axis_index("ep"), place]).astype(jnp.int32)
    partial_rows = shared_kernel(where, line, pair, own, far, swap, side)
    partial_back = lax.all_to_all(
        partial_rows.reshape(group, per_dev, width),
        "ep",
        split_axis=0,
        concat_axis=0,
        axis_index_groups=[list(range(g, g + group)) for g in range(0, ep_count, group)],
        tiled=True,
    )
    shared = jnp.sum(partial_back.astype(f32), axis=0)

    both = lax.dot_general(
        share,
        jnp.concatenate([returned, returned], axis=0),
        (((0,), (0,)), ((), ())),
        preferred_element_type=f32,
    )
    half = per_dev * chips
    theirs = lax.ppermute(both[half:].astype(bf16), "tp", core_swap(tp_count))
    pair = both[:half] + theirs.astype(f32)
    routed = pair[:per_dev]
    pair = pair.astype(bf16)
    for step in range(1, chips):
        routed = routed + lax.ppermute(
            pair[step * per_dev : (step + 1) * per_dev], "tp", y_shift(tp_count, step)
        ).astype(f32)
    gate_value = jax.nn.sigmoid(jnp.dot(own_mid, gate_vector, preferred_element_type=f32))
    layer_out = (own_after + routed + gate_value[:, None] * shared).astype(bf16)
    return (layer_out, new_state)


def solution(mesh):
    return jax.shard_map(
        layer,
        mesh=mesh,
        in_specs=(
            P("ep", "tp"),
            P(),
            P(None, "tp"),
            P(None, "ep", "tp"),
            P("tp", None),
            P("tp", None),
            P("tp"),
            P(None, "tp", None, None),
            P(None, "tp", None, None),
            P("tp"),
            P(),
            P(),
            P(),
            P("ep", None),
            P("ep", None),
            P(("ep", "tp"), None, None),
            P(("ep", "tp"), None, None),
            P(("ep", "tp"), None, None),
            P(None, "ep"),
            P(None, "ep"),
            P("ep", None),
        ),
        out_specs=(P(("ep", "tp"), None), P(None, "ep", "tp")),
        check_vma=False,
    )
```

```python
import functools
import math

import jax
import jax.numpy as jnp
from jax import lax
from jax.experimental import pallas as pl
from jax.experimental.pallas import tpu as pltpu
from jax.sharding import PartitionSpec as P


norm_eps = 1e-05
routed_scale = 2.5
f32 = jnp.float32
bf16 = jnp.bfloat16
cores = 2


def y_shift(tp_count, step):
    chips = tp_count // cores
    return [
        (y * cores + c, ((y + step) % chips) * cores + c)
        for y in range(chips)
        for c in range(cores)
    ]


def core_swap(tp_count):
    return [(i, i ^ 1) for i in range(tp_count)]


def hop_gather(array, tp_count):
    chips = tp_count // cores
    mine = [array] + [
        lax.ppermute(array, "tp", y_shift(tp_count, step)) for step in range(1, chips)
    ]
    other = [lax.ppermute(part, "tp", core_swap(tp_count)) for part in mine]
    return mine, other


def plane_shift(ep_count, z_step, x_step):
    side = math.isqrt(ep_count)
    return [
        (z * side + x, ((z + z_step) % side) * side + (x + x_step) % side)
        for z in range(side)
        for x in range(side)
    ]


def weight_moves(ep_count, tp_count, core):
    side = math.isqrt(ep_count)
    moves = []
    for e in range(ep_count):
        far = (side - 1 - e // side) * side + e % side
        for t in range(tp_count):
            to = far if t % cores == core else e
            moves.append((e * tp_count + t, to * tp_count + (t ^ 1)))
    return moves


def pair_swap(ep_count):
    side = math.isqrt(ep_count)
    return [(e, ((e // side) ^ 1) * side + e % side) for e in range(ep_count)]


def natural_blocks(mine, other, tp_count, place):
    chips = tp_count // cores
    y, c = place // cores, place % cores
    even = jnp.where(c == 0, mine, other)
    odd = jnp.where(c == 0, other, mine)
    blocks = []
    for b in range(tp_count):
        k = (y - b // cores) % chips
        blocks.append(lax.dynamic_index_in_dim(even if b % cores == 0 else odd, k, 0, False))
    return jnp.concatenate(blocks, axis=1)


def layer_norm(values, gain_vec):
    row_mean = jnp.mean(values, axis=-1, keepdims=True)
    row_square = jnp.mean(values * values, axis=-1, keepdims=True)
    return (values - row_mean) * lax.rsqrt(row_square - row_mean * row_mean + norm_eps) * gain_vec


def coefficients(decay_rate, frequency, log_step, in_coef):
    time_step = jnp.exp(log_step)[:, None]
    real_rate = -decay_rate
    magnitude = jnp.exp(real_rate * time_step)
    keep_re = magnitude * jnp.cos(frequency * time_step)
    keep_im = magnitude * jnp.sin(frequency * time_step)
    denominator = real_rate * real_rate + frequency * frequency
    factor_re = ((keep_re - 1.0) * real_rate + keep_im * frequency) / denominator
    factor_im = (keep_im * real_rate - (keep_re - 1.0) * frequency) / denominator
    push_re = factor_re[..., None] * in_coef[0] - factor_im[..., None] * in_coef[1]
    push_im = factor_re[..., None] * in_coef[1] + factor_im[..., None] * in_coef[0]
    return (keep_re, keep_im, push_re, push_im)


def mixer_step(
    normed, in_weight, state, decay_rate, frequency, log_step, in_coef, out_coef, skip_gain
):
    row_count = normed.shape[0]
    group_count, state_count = decay_rate.shape
    keep_re, keep_im, push_re, push_im = coefficients(decay_rate, frequency, log_step, in_coef)
    drive = jnp.dot(normed, in_weight, preferred_element_type=f32).astype(bf16)
    drive_f = drive.astype(f32).reshape(row_count, group_count, -1)
    input_re = jnp.einsum("tgh,gph->tgp", drive_f, push_re)
    input_im = jnp.einsum("tgh,gph->tgp", drive_f, push_im)
    old_re = state[0].reshape(row_count, group_count, state_count)
    old_im = state[1].reshape(row_count, group_count, state_count)
    new_re = keep_re * old_re - keep_im * old_im + input_re
    new_im = keep_re * old_im + keep_im * old_re + input_im
    read_out = jnp.einsum("ghp,tgp->tgh", out_coef[0], new_re) - jnp.einsum(
        "ghp,tgp->tgh", out_coef[1], new_im
    )
    read_out = read_out.reshape(row_count, -1) + skip_gain * drive_f.reshape(row_count, -1)
    mixed_rows = jax.nn.gelu(read_out, approximate=True).astype(bf16)
    updated = jnp.stack([new_re.reshape(row_count, -1), new_im.reshape(row_count, -1)])
    return (mixed_rows, updated)


def in_hbm():
    return pl.BlockSpec(memory_space=pltpu.HBM)


def in_vmem():
    return pl.BlockSpec(memory_space=pltpu.VMEM)


def in_smem():
    return pl.BlockSpec(memory_space=pltpu.SMEM)


def mm(a, b):
    return jnp.dot(a, b, preferred_element_type=f32)


def expert_body(
    rows_hbm, gate_hbm, up_hbm, down_hbm, out_hbm, rows, gate, up, down, hidden, out, sems
):
    cuts, depth = gate.shape[0], gate.shape[1]
    halves = down.shape[0]
    load_rows = pltpu.make_async_copy(rows_hbm, rows, sems.at[0])
    load_rows.start()
    loads = []
    for i in range(cuts):
        pair = (
            pltpu.make_async_copy(gate_hbm.at[i], gate.at[i], sems.at[1 + 2 * i]),
            pltpu.make_async_copy(up_hbm.at[i], up.at[i], sems.at[2 + 2 * i]),
        )
        for copy in pair:
            copy.start()
        loads.append(pair)
    span = down.shape[2]
    tail = [
        pltpu.make_async_copy(
            down_hbm.at[:, i * span : (i + 1) * span], down.at[i], sems.at[1 + 2 * cuts + i]
        )
        for i in range(halves)
    ]
    for copy in tail:
        copy.start()
    load_rows.wait()
    gate_part = up_part = None
    for i in range(cuts):
        for copy in loads[i]:
            copy.wait()
        block = rows[:, i * depth : (i + 1) * depth]
        g, u = mm(block, gate[i]), mm(block, up[i])
        gate_part = g if gate_part is None else gate_part + g
        up_part = u if up_part is None else up_part + u
    hidden[...] = (gate_part * jax.nn.sigmoid(gate_part) * up_part).astype(bf16)
    stores = []
    for i in range(halves):
        tail[i].wait()
        out[i] = mm(hidden[...], down[i]).astype(bf16)
        store = pltpu.make_async_copy(
            out.at[i], out_hbm.at[:, i * span : (i + 1) * span], sems.at[1 + 2 * i]
        )
        store.start()
        stores.append(store)
    for store in stores:
        store.wait()


def expert_kernel(rows, gate, up, down):
    count, width = rows.shape
    inner = gate.shape[1]
    cuts, parts = 8, 2
    return pl.pallas_call(
        expert_body,
        out_shape=jax.ShapeDtypeStruct((count, width), bf16),
        in_specs=[in_hbm()] * 4,
        out_specs=in_hbm(),
        scratch_shapes=[
            pltpu.VMEM((count, width), bf16),
            pltpu.VMEM((cuts, width // cuts, inner), bf16),
            pltpu.VMEM((cuts, width // cuts, inner), bf16),
            pltpu.VMEM((parts, inner, width // parts), bf16),
            pltpu.VMEM((count, inner), bf16),
            pltpu.VMEM((parts, count, width // parts), bf16),
            pltpu.SemaphoreType.DMA((1 + 2 * cuts + parts,)),
        ],
        compiler_params=pltpu.CompilerParams(vmem_limit_bytes=60 * 1024 * 1024),
        name="expert_mlp",
    )(
        rows,
        gate.reshape(cuts, width // cuts, inner),
        up.reshape(cuts, width // cuts, inner),
        down,
    )


def shared_body(
    here,
    place,
    line_hbm,
    pair_hbm,
    gate_hbm,
    up_hbm,
    down_hbm,
    gate_far,
    up_far,
    down_far,
    gate_swap,
    up_swap,
    down_swap,
    out_hbm,
    gate,
    up,
    down,
    rows,
    out,
    sems,
    *,
    side,
):
    core = lax.rem(place[0], cores)
    z, x = lax.rem(lax.div(here[0], side), 2), lax.rem(here[0], side)
    order = [
        lax.rem(z + i, 2) * side + lax.rem(x + side - j, side) for i in range(2) for j in range(side)
    ]
    moves = [
        pltpu.make_async_copy(line_hbm, rows.at[0], sems.at[0]),
        pltpu.make_async_copy(pair_hbm, rows.at[1], sems.at[1]),
    ]
    near = [
        pltpu.make_async_copy(source, target.at[0], sems.at[2 + i])
        for i, (source, target) in enumerate(((gate_hbm, gate), (up_hbm, up), (down_hbm, down)))
    ]
    for copy in moves + near:
        copy.start()

    @pl.when(core == 0)
    def _():
        pltpu.make_async_copy(gate_swap, gate.at[1], sems.at[5]).start()
        pltpu.make_async_copy(up_far, up.at[1], sems.at[6]).start()
        pltpu.make_async_copy(down_swap, down.at[1], sems.at[7]).start()

    @pl.when(core != 0)
    def _():
        pltpu.make_async_copy(gate_far, gate.at[1], sems.at[5]).start()
        pltpu.make_async_copy(up_swap, up.at[1], sems.at[6]).start()
        pltpu.make_async_copy(down_far, down.at[1], sems.at[7]).start()

    far = [
        pltpu.make_async_copy(gate_far, gate.at[1], sems.at[5]),
        pltpu.make_async_copy(up_far, up.at[1], sems.at[6]),
        pltpu.make_async_copy(down_far, down.at[1], sems.at[7]),
    ]
    for copy in moves:
        copy.wait()
    count = 2 * rows.shape[1]
    x_all = rows[...].reshape(count, rows.shape[2])
    hidden = []
    for i, loads in enumerate((near, far)):
        loads[0].wait()
        gate_part = mm(x_all, gate[i])
        loads[1].wait()
        up_part = mm(x_all, up[i])
        hidden.append((gate_part * jax.nn.sigmoid(gate_part) * up_part).astype(bf16))
    near[2].wait()
    far[2].wait()
    per = rows.shape[1] // side
    stores = []
    for half in range(2):
        lo = half * count // 2
        part = slice(lo, lo + count // 2)
        total = mm(hidden[0][part], down[0]) + mm(hidden[1][part], down[1])
        out[part, :] = total.astype(bf16)
        for k in range(half * side, (half + 1) * side):
            at = pl.multiple_of(order[k] * per, per)
            stores.append(
                pltpu.make_async_copy(
                    out.at[k * per : (k + 1) * per, :], out_hbm.at[pl.ds(at, per), :], sems.at[8 + k]
                )
            )
            stores[-1].start()
    for store in stores:
        store.wait()


def shared_kernel(here, place, line, pair, own, far, swap, side):
    count, width = line.shape
    inner = own[0].shape[1]
    return pl.pallas_call(
        functools.partial(shared_body, side=side),
        out_shape=jax.ShapeDtypeStruct((count * 2, width), bf16),
        in_specs=[in_smem()] * 2 + [in_hbm()] * 11,
        out_specs=in_hbm(),
        scratch_shapes=[
            pltpu.VMEM((2, width, inner), bf16),
            pltpu.VMEM((2, width, inner), bf16),
            pltpu.VMEM((2, inner, width), bf16),
            pltpu.VMEM((2, count, width), bf16),
            pltpu.VMEM((count * 2, width), bf16),
            pltpu.SemaphoreType.DMA((8 + 2 * side,)),
        ],
        compiler_params=pltpu.CompilerParams(vmem_limit_bytes=60 * 1024 * 1024),
        name="shared_mlp",
    )(here, place, line, pair, *own, *far, *swap)


def pull_body(weight_hbm, out, sem):
    copy = pltpu.make_async_copy(weight_hbm, out, sem)
    copy.start()
    copy.wait()


def pull_kernel(weight):
    return pl.pallas_call(
        pull_body,
        out_shape=jax.ShapeDtypeStruct(weight.shape, weight.dtype),
        in_specs=[in_hbm()],
        out_specs=in_vmem(),
        scratch_shapes=[pltpu.SemaphoreType.DMA(())],
        compiler_params=pltpu.CompilerParams(vmem_limit_bytes=8 << 20),
        name="pull_weight",
    )(weight)


def mid_body(place, *refs, tp):
    resid, mixed, refs = refs[:tp], refs[tp : 2 * tp], refs[2 * tp :]
    chips = tp // cores
    chip, core = lax.div(place[0], cores), lax.rem(place[0], cores)
    order = [
        lax.rem(chip + chips - k, chips) * cores + (core ^ other)
        for other in range(cores)
        for k in range(chips)
    ]
    weight, gain, picked, own_mid, after_hbm, outgoing_hbm, rows, total, normed, outgoing, sems = refs
    feat, chan = resid[0].shape[1], mixed[0].shape[1]
    for i in range(tp):
        at = pl.multiple_of(order[i] * feat, feat)
        total[:, pl.ds(at, feat)] = resid[i][...].astype(f32)
        at = pl.multiple_of(order[i] * chan, chan)
        rows[:, pl.ds(at, chan)] = mixed[i][...]
    total[...] += mm(rows[...], weight[...])
    values = total[...]
    mean = jnp.mean(values, axis=-1, keepdims=True)
    square = jnp.mean(values * values, axis=-1, keepdims=True)
    scale = lax.rsqrt(square - mean * mean + norm_eps)
    normed[...] = ((values - mean) * scale * gain[...]).astype(bf16)
    per = own_mid.shape[0]
    at = pl.multiple_of(place[0] * per, per)
    own_mid[...] = normed[pl.ds(at, per), :]
    keep = pltpu.make_async_copy(total.at[pl.ds(at, per), :], after_hbm, sems.at[0])
    keep.start()
    outgoing[...] = mm(picked[...], normed[...]).astype(bf16)
    store = pltpu.make_async_copy(outgoing, outgoing_hbm, sems.at[1])
    store.start()
    keep.wait()
    store.wait()


def mid_kernel(place, resid, mixed, weight, gain, picked):
    tp = len(resid)
    rows, feat = resid[0].shape
    chan = mixed[0].shape[1]
    width = feat * tp
    per = rows // tp
    return pl.pallas_call(
        functools.partial(mid_body, tp=tp),
        out_shape=(
            jax.ShapeDtypeStruct((per, width), bf16),
            jax.ShapeDtypeStruct((per, width), f32),
            jax.ShapeDtypeStruct((picked.shape[0], width), bf16),
        ),
        in_specs=[in_smem()] + [in_vmem()] * (2 * tp + 3),
        out_specs=(in_vmem(), in_hbm(), in_hbm()),
        scratch_shapes=[
            pltpu.VMEM((rows, chan * tp), bf16),
            pltpu.VMEM((rows, width), f32),
            pltpu.VMEM((rows, width), bf16),
            pltpu.VMEM((picked.shape[0], width), bf16),
            pltpu.SemaphoreType.DMA((2,)),
        ],
        compiler_params=pltpu.CompilerParams(vmem_limit_bytes=24 << 20),
        name="out_proj_norm",
    )(
        place,
        *resid,
        *mixed,
        weight,
        gain.reshape(1, width),
        picked,
    )


def join_body(*refs):
    parts, out, sems = refs[:-2], refs[-2], refs[-1]
    per = parts[0].shape[0]
    moves = [
        pltpu.make_async_copy(part, out.at[pl.ds(i * per, per), :], sems.at[i])
        for i, part in enumerate(parts)
    ]
    for copy in moves:
        copy.start()
    for copy in moves:
        copy.wait()


def join_kernel(parts):
    per, width = parts[0].shape
    return pl.pallas_call(
        join_body,
        out_shape=jax.ShapeDtypeStruct((per * len(parts), width), parts[0].dtype),
        in_specs=[in_vmem()] * len(parts),
        out_specs=in_hbm(),
        scratch_shapes=[pltpu.SemaphoreType.DMA((len(parts),))],
        compiler_params=pltpu.CompilerParams(vmem_limit_bytes=8 << 20),
        name="join_rows",
    )(*parts)


def tables_body(place, routes, weights, picked_out, share_out, *, experts, tp_count):
    top, rows = routes.shape
    slots = picked_out.shape[0]
    capacity = slots * tp_count // experts
    tp = place[0]
    chips = tp_count // cores
    per = rows // tp_count
    slot = lax.broadcasted_iota(jnp.int32, (slots, rows), 0)
    wanted = (slot // capacity) * tp_count + tp
    total = jnp.sum(weights[...], axis=0, keepdims=True)
    named = routes[0:1, :] == wanted
    share = jnp.where(named, weights[0:1, :] / total * routed_scale, 0.0)
    for j in range(1, top):
        hit = routes[j : j + 1, :] == wanted
        named = named | hit
        share = share + jnp.where(hit, weights[j : j + 1, :] / total * routed_scale, 0.0)
    down = lax.broadcasted_iota(jnp.int32, (rows, rows), 0)
    across = lax.broadcasted_iota(jnp.int32, (rows, rows), 1)
    rank = mm(named.astype(f32).astype(bf16), (down < across).astype(f32).astype(bf16))
    picked = named & (rank == (slot % capacity).astype(f32))
    picked_out[...] = jnp.where(picked, 1.0, 0.0).astype(bf16)
    share = jnp.where(picked, share, 0.0)
    high = share.astype(bf16)
    low = (share - high.astype(f32)).astype(bf16)
    ahead = (across // per) % chips
    core = (tp % cores) ^ (across // (per * chips))
    source = (((tp // cores + ahead) % chips) * cores + core) * per + across % per
    turn = (source == down).astype(f32).astype(bf16)
    share_out[:slots, :] = mm(high, turn).astype(bf16)
    share_out[slots:, :] = mm(low, turn).astype(bf16)


def tables_kernel(place, routes, weights, experts, tp_count):
    rows, top = routes.shape
    slots = max(2, 2 * rows * top // experts) * (experts // tp_count)
    return pl.pallas_call(
        functools.partial(tables_body, experts=experts, tp_count=tp_count),
        out_shape=(
            jax.ShapeDtypeStruct((slots, rows), bf16),
            jax.ShapeDtypeStruct((2 * slots, rows), bf16),
        ),
        in_specs=[in_smem()] + [in_vmem()] * 2,
        out_specs=(in_vmem(),) * 2,
        compiler_params=pltpu.CompilerParams(vmem_limit_bytes=8 << 20),
        name="slot_tables",
    )(place, routes.T, weights.T)


def layer(
    residual,
    in_gain,
    in_weight,
    state,
    decay_rate,
    frequency,
    log_step,
    in_coef,
    out_coef,
    skip_gain,
    out_weight,
    mid_gain,
    gate_vector,
    routes,
    route_weight,
    expert_gate,
    expert_up,
    expert_down,
    shared_gate,
    shared_up,
    shared_down,
):
    tp_count = lax.axis_size("tp")
    ep_count = lax.axis_size("ep")
    chips = tp_count // cores
    place = lax.axis_index("tp")
    seq_rows, feat_part = residual.shape
    width = feat_part * tp_count
    per_dev = seq_rows // tp_count
    capacity = max(2, 2 * seq_rows * routes.shape[1] // (ep_count * tp_count))
    slots = ep_count * capacity

    resid_mine, resid_other = hop_gather(residual, tp_count)
    own = (shared_gate, shared_up, shared_down)
    far = []
    for w, core in zip(own, (0, 1, 0)):
        far.append(lax.ppermute(w, ("ep", "tp"), weight_moves(ep_count, tp_count, core)))
    swap = [lax.ppermute(w, "tp", core_swap(tp_count)) for w in far]
    full_resid = natural_blocks(jnp.stack(resid_mine), jnp.stack(resid_other), tp_count, place).astype(f32)
    normed = layer_norm(full_resid, in_gain).astype(bf16)
    mixed_part, new_state = mixer_step(
        normed, in_weight, state, decay_rate, frequency, log_step, in_coef, out_coef, skip_gain
    )
    picked, share = tables_kernel(
        place.reshape(1), routes, route_weight, ep_count * tp_count, tp_count
    )
    mixed_mine, mixed_other = hop_gather(mixed_part, tp_count)
    out_rows = pull_kernel(out_weight)
    own_mid, own_after, outgoing = mid_kernel(
        place.reshape(1), resid_mine + resid_other, mixed_mine + mixed_other, out_rows, mid_gain, picked
    )

    side = math.isqrt(ep_count)
    line = [own_mid]
    for step in range(1, side):
        line.append(lax.ppermute(own_mid, "ep", plane_shift(ep_count, 0, step)))
    line = join_kernel(line)
    pair = lax.ppermute(line, "ep", pair_swap(ep_count))
    slot_rows = lax.all_to_all(
        outgoing.reshape(ep_count, capacity, width), "ep", split_axis=0, concat_axis=0, tiled=True
    ).reshape(slots, width)

    result = expert_kernel(slot_rows, expert_gate[0], expert_up[0], expert_down[0])
    returned = lax.all_to_all(
        result.reshape(ep_count, capacity, width), "ep", split_axis=0, concat_axis=0, tiled=True
    ).reshape(slots, width)

    group = 2 * side
    partial_rows = shared_kernel(
        lax.axis_index("ep").reshape(1), place.reshape(1), line, pair, own, far, swap, side
    )
    partial_back = lax.all_to_all(
        partial_rows.reshape(group, per_dev, width),
        "ep",
        split_axis=0,
        concat_axis=0,
        axis_index_groups=[list(range(g, g + group)) for g in range(0, ep_count, group)],
        tiled=True,
    )
    shared = jnp.sum(partial_back.astype(f32), axis=0)

    half = per_dev * chips
    doubled = jnp.concatenate([returned, returned], axis=0)
    send, keep = (
        lax.dot_general(
            part, doubled, (((0,), (0,)), ((), ())), preferred_element_type=f32
        ).astype(bf16)
        for part in (share[:, half:], share[:, :half])
    )
    theirs = lax.ppermute(send, "tp", core_swap(tp_count))
    pair = keep.astype(f32) + theirs.astype(f32)
    routed = pair[:per_dev]
    pair = pair.astype(bf16)
    for step in range(1, chips):
        routed = routed + lax.ppermute(
            pair[step * per_dev : (step + 1) * per_dev], "tp", y_shift(tp_count, step)
        ).astype(f32)
    gate_value = jax.nn.sigmoid(jnp.dot(own_mid, gate_vector, preferred_element_type=f32))
    layer_out = (own_after + routed + gate_value[:, None] * shared).astype(bf16)
    return (layer_out, new_state)


def solution(mesh):
    return jax.shard_map(
        layer,
        mesh=mesh,
        in_specs=(
            P("ep", "tp"),
            P(),
            P(None, "tp"),
            P(None, "ep", "tp"),
            P("tp", None),
            P("tp", None),
            P("tp"),
            P(None, "tp", None, None),
            P(None, "tp", None, None),
            P("tp"),
            P(),
            P(),
            P(),
            P("ep", None),
            P("ep", None),
            P(("ep", "tp"), None, None),
            P(("ep", "tp"), None, None),
            P(("ep", "tp"), None, None),
            P(None, "ep"),
            P(None, "ep"),
            P("ep", None),
        ),
        out_specs=(P(("ep", "tp"), None), P(None, "ep", "tp")),
        check_vma=False,
    )
```

```python
import functools
import math

import jax
import jax.numpy as jnp
from jax import lax
from jax.experimental import pallas as pl
from jax.experimental.pallas import tpu as pltpu
from jax.sharding import PartitionSpec as P


norm_eps = 1e-05
routed_scale = 2.5
f32 = jnp.float32
bf16 = jnp.bfloat16
cores = 2


def y_shift(tp_count, step):
    chips = tp_count // cores
    return [
        (y * cores + c, ((y + step) % chips) * cores + c)
        for y in range(chips)
        for c in range(cores)
    ]


def core_swap(tp_count):
    return [(i, i ^ 1) for i in range(tp_count)]


def hop_gather(array, tp_count):
    chips = tp_count // cores
    mine = [array] + [
        lax.ppermute(array, "tp", y_shift(tp_count, step)) for step in range(1, chips)
    ]
    other = [lax.ppermute(part, "tp", core_swap(tp_count)) for part in mine]
    return mine, other


def plane_shift(ep_count, z_step, x_step):
    side = math.isqrt(ep_count)
    return [
        (z * side + x, ((z + z_step) % side) * side + (x + x_step) % side)
        for z in range(side)
        for x in range(side)
    ]


def weight_moves(ep_count, tp_count, core):
    side = math.isqrt(ep_count)
    moves = []
    for e in range(ep_count):
        far = (side - 1 - e // side) * side + e % side
        for t in range(tp_count):
            to = far if t % cores == core else e
            moves.append((e * tp_count + t, to * tp_count + (t ^ 1)))
    return moves


def pair_swap(ep_count):
    side = math.isqrt(ep_count)
    return [(e, ((e // side) ^ 1) * side + e % side) for e in range(ep_count)]


def natural_blocks(mine, other, tp_count, place):
    chips = tp_count // cores
    y, c = place // cores, place % cores
    even = jnp.where(c == 0, mine, other)
    odd = jnp.where(c == 0, other, mine)
    blocks = []
    for b in range(tp_count):
        k = (y - b // cores) % chips
        blocks.append(lax.dynamic_index_in_dim(even if b % cores == 0 else odd, k, 0, False))
    return jnp.concatenate(blocks, axis=1)


def layer_norm(values, gain_vec):
    row_mean = jnp.mean(values, axis=-1, keepdims=True)
    row_square = jnp.mean(values * values, axis=-1, keepdims=True)
    return (values - row_mean) * lax.rsqrt(row_square - row_mean * row_mean + norm_eps) * gain_vec


def coefficients(decay_rate, frequency, log_step, in_coef):
    time_step = jnp.exp(log_step)[:, None]
    real_rate = -decay_rate
    magnitude = jnp.exp(real_rate * time_step)
    keep_re = magnitude * jnp.cos(frequency * time_step)
    keep_im = magnitude * jnp.sin(frequency * time_step)
    denominator = real_rate * real_rate + frequency * frequency
    factor_re = ((keep_re - 1.0) * real_rate + keep_im * frequency) / denominator
    factor_im = (keep_im * real_rate - (keep_re - 1.0) * frequency) / denominator
    push_re = factor_re[..., None] * in_coef[0] - factor_im[..., None] * in_coef[1]
    push_im = factor_re[..., None] * in_coef[1] + factor_im[..., None] * in_coef[0]
    return (keep_re, keep_im, push_re, push_im)


def mixer_step(
    normed, in_weight, state, decay_rate, frequency, log_step, in_coef, out_coef, skip_gain
):
    row_count = normed.shape[0]
    group_count, state_count = decay_rate.shape
    keep_re, keep_im, push_re, push_im = coefficients(decay_rate, frequency, log_step, in_coef)
    drive = jnp.dot(normed, in_weight, preferred_element_type=f32).astype(bf16)
    drive_f = drive.astype(f32).reshape(row_count, group_count, -1)
    input_re = jnp.einsum("tgh,gph->tgp", drive_f, push_re)
    input_im = jnp.einsum("tgh,gph->tgp", drive_f, push_im)
    old_re = state[0].reshape(row_count, group_count, state_count)
    old_im = state[1].reshape(row_count, group_count, state_count)
    new_re = keep_re * old_re - keep_im * old_im + input_re
    new_im = keep_re * old_im + keep_im * old_re + input_im
    read_out = jnp.einsum("ghp,tgp->tgh", out_coef[0], new_re) - jnp.einsum(
        "ghp,tgp->tgh", out_coef[1], new_im
    )
    read_out = read_out.reshape(row_count, -1) + skip_gain * drive_f.reshape(row_count, -1)
    mixed_rows = jax.nn.gelu(read_out, approximate=True).astype(bf16)
    updated = jnp.stack([new_re.reshape(row_count, -1), new_im.reshape(row_count, -1)])
    return (mixed_rows, updated)


def in_hbm():
    return pl.BlockSpec(memory_space=pltpu.HBM)


def in_vmem():
    return pl.BlockSpec(memory_space=pltpu.VMEM)


def in_smem():
    return pl.BlockSpec(memory_space=pltpu.SMEM)


def mm(a, b):
    return jnp.dot(a, b, preferred_element_type=f32)


def expert_body(
    rows_hbm, gate_hbm, up_hbm, down_hbm, out_hbm, rows, gate, up, down, hidden, out, sems
):
    cuts, depth = gate.shape[0], gate.shape[1]
    halves = down.shape[0]
    load_rows = pltpu.make_async_copy(rows_hbm, rows, sems.at[0])
    load_rows.start()
    loads = []
    for i in range(cuts):
        pair = (
            pltpu.make_async_copy(gate_hbm.at[i], gate.at[i], sems.at[1 + 2 * i]),
            pltpu.make_async_copy(up_hbm.at[i], up.at[i], sems.at[2 + 2 * i]),
        )
        for copy in pair:
            copy.start()
        loads.append(pair)
    span = down.shape[2]
    tail = [
        pltpu.make_async_copy(
            down_hbm.at[:, i * span : (i + 1) * span], down.at[i], sems.at[1 + 2 * cuts + i]
        )
        for i in range(halves)
    ]
    for copy in tail:
        copy.start()
    load_rows.wait()
    gate_part = up_part = None
    for i in range(cuts):
        for copy in loads[i]:
            copy.wait()
        block = rows[:, i * depth : (i + 1) * depth]
        g, u = mm(block, gate[i]), mm(block, up[i])
        gate_part = g if gate_part is None else gate_part + g
        up_part = u if up_part is None else up_part + u
    hidden[...] = (gate_part * jax.nn.sigmoid(gate_part) * up_part).astype(bf16)
    stores = []
    for i in range(halves):
        tail[i].wait()
        out[i] = mm(hidden[...], down[i]).astype(bf16)
        store = pltpu.make_async_copy(
            out.at[i], out_hbm.at[:, i * span : (i + 1) * span], sems.at[1 + 2 * i]
        )
        store.start()
        stores.append(store)
    for store in stores:
        store.wait()


def expert_kernel(rows, gate, up, down):
    count, width = rows.shape
    inner = gate.shape[1]
    cuts, parts = 8, 2
    return pl.pallas_call(
        expert_body,
        out_shape=jax.ShapeDtypeStruct((count, width), bf16),
        in_specs=[in_hbm()] * 4,
        out_specs=in_hbm(),
        scratch_shapes=[
            pltpu.VMEM((count, width), bf16),
            pltpu.VMEM((cuts, width // cuts, inner), bf16),
            pltpu.VMEM((cuts, width // cuts, inner), bf16),
            pltpu.VMEM((parts, inner, width // parts), bf16),
            pltpu.VMEM((count, inner), bf16),
            pltpu.VMEM((parts, count, width // parts), bf16),
            pltpu.SemaphoreType.DMA((1 + 2 * cuts + parts,)),
        ],
        compiler_params=pltpu.CompilerParams(vmem_limit_bytes=60 * 1024 * 1024),
        name="expert_mlp",
    )(
        rows,
        gate.reshape(cuts, width // cuts, inner),
        up.reshape(cuts, width // cuts, inner),
        down,
    )


def shared_body(
    here,
    place,
    line_hbm,
    pair_hbm,
    gate_hbm,
    up_hbm,
    down_hbm,
    gate_far,
    up_far,
    down_far,
    gate_swap,
    up_swap,
    down_swap,
    out_hbm,
    gate,
    up,
    down,
    rows,
    out,
    sems,
    *,
    side,
):
    core = lax.rem(place[0], cores)
    z, x = lax.rem(lax.div(here[0], side), 2), lax.rem(here[0], side)
    order = [
        lax.rem(z + i, 2) * side + lax.rem(x + side - j, side) for i in range(2) for j in range(side)
    ]
    moves = [
        pltpu.make_async_copy(line_hbm, rows.at[0], sems.at[0]),
        pltpu.make_async_copy(pair_hbm, rows.at[1], sems.at[1]),
    ]
    near = [
        pltpu.make_async_copy(source, target.at[0], sems.at[2 + i])
        for i, (source, target) in enumerate(((gate_hbm, gate), (up_hbm, up), (down_hbm, down)))
    ]
    for copy in moves + near:
        copy.start()

    @pl.when(core == 0)
    def _():
        pltpu.make_async_copy(gate_swap, gate.at[1], sems.at[5]).start()
        pltpu.make_async_copy(up_far, up.at[1], sems.at[6]).start()
        pltpu.make_async_copy(down_swap, down.at[1], sems.at[7]).start()

    @pl.when(core != 0)
    def _():
        pltpu.make_async_copy(gate_far, gate.at[1], sems.at[5]).start()
        pltpu.make_async_copy(up_swap, up.at[1], sems.at[6]).start()
        pltpu.make_async_copy(down_far, down.at[1], sems.at[7]).start()

    far = [
        pltpu.make_async_copy(gate_far, gate.at[1], sems.at[5]),
        pltpu.make_async_copy(up_far, up.at[1], sems.at[6]),
        pltpu.make_async_copy(down_far, down.at[1], sems.at[7]),
    ]
    for copy in moves:
        copy.wait()
    count = 2 * rows.shape[1]
    x_all = rows[...].reshape(count, rows.shape[2])
    hidden = []
    for i, loads in enumerate((near, far)):
        loads[0].wait()
        gate_part = mm(x_all, gate[i])
        loads[1].wait()
        up_part = mm(x_all, up[i])
        hidden.append((gate_part * jax.nn.sigmoid(gate_part) * up_part).astype(bf16))
    near[2].wait()
    far[2].wait()
    per = rows.shape[1] // side
    stores = []
    for half in range(2):
        lo = half * count // 2
        part = slice(lo, lo + count // 2)
        total = mm(hidden[0][part], down[0]) + mm(hidden[1][part], down[1])
        out[part, :] = total.astype(bf16)
        for k in range(half * side, (half + 1) * side):
            at = pl.multiple_of(order[k] * per, per)
            stores.append(
                pltpu.make_async_copy(
                    out.at[k * per : (k + 1) * per, :], out_hbm.at[pl.ds(at, per), :], sems.at[8 + k]
                )
            )
            stores[-1].start()
    for store in stores:
        store.wait()


def shared_kernel(here, place, line, pair, own, far, swap, side):
    count, width = line.shape
    inner = own[0].shape[1]
    return pl.pallas_call(
        functools.partial(shared_body, side=side),
        out_shape=jax.ShapeDtypeStruct((count * 2, width), bf16),
        in_specs=[in_smem()] * 2 + [in_hbm()] * 11,
        out_specs=in_hbm(),
        scratch_shapes=[
            pltpu.VMEM((2, width, inner), bf16),
            pltpu.VMEM((2, width, inner), bf16),
            pltpu.VMEM((2, inner, width), bf16),
            pltpu.VMEM((2, count, width), bf16),
            pltpu.VMEM((count * 2, width), bf16),
            pltpu.SemaphoreType.DMA((8 + 2 * side,)),
        ],
        compiler_params=pltpu.CompilerParams(vmem_limit_bytes=60 * 1024 * 1024),
        name="shared_mlp",
    )(here, place, line, pair, *own, *far, *swap)


def pull_body(weight_hbm, out, sem):
    copy = pltpu.make_async_copy(weight_hbm, out, sem)
    copy.start()
    copy.wait()


def pull_kernel(weight):
    return pl.pallas_call(
        pull_body,
        out_shape=jax.ShapeDtypeStruct(weight.shape, weight.dtype),
        in_specs=[in_hbm()],
        out_specs=in_vmem(),
        scratch_shapes=[pltpu.SemaphoreType.DMA(())],
        compiler_params=pltpu.CompilerParams(vmem_limit_bytes=8 << 20),
        name="pull_weight",
    )(weight)


def mid_body(place, *refs, tp):
    resid, mixed, refs = refs[:tp], refs[tp : 2 * tp], refs[2 * tp :]
    chips = tp // cores
    chip, core = lax.div(place[0], cores), lax.rem(place[0], cores)
    order = [
        lax.rem(chip + chips - k, chips) * cores + (core ^ other)
        for other in range(cores)
        for k in range(chips)
    ]
    weight, gain, picked, own_mid, after_hbm, outgoing_hbm, rows, total, normed, outgoing, sems = refs
    feat, chan = resid[0].shape[1], mixed[0].shape[1]
    for i in range(tp):
        at = pl.multiple_of(order[i] * feat, feat)
        total[:, pl.ds(at, feat)] = resid[i][...].astype(f32)
        at = pl.multiple_of(order[i] * chan, chan)
        rows[:, pl.ds(at, chan)] = mixed[i][...]
    total[...] += mm(rows[...], weight[...])
    values = total[...]
    mean = jnp.mean(values, axis=-1, keepdims=True)
    square = jnp.mean(values * values, axis=-1, keepdims=True)
    scale = lax.rsqrt(square - mean * mean + norm_eps)
    normed[...] = ((values - mean) * scale * gain[...]).astype(bf16)
    per = own_mid.shape[0]
    at = pl.multiple_of(place[0] * per, per)
    own_mid[...] = normed[pl.ds(at, per), :]
    keep = pltpu.make_async_copy(total.at[pl.ds(at, per), :], after_hbm, sems.at[0])
    keep.start()
    outgoing[...] = mm(picked[...], normed[...]).astype(bf16)
    store = pltpu.make_async_copy(outgoing, outgoing_hbm, sems.at[1])
    store.start()
    keep.wait()
    store.wait()


def mid_kernel(place, resid, mixed, weight, gain, picked):
    tp = len(resid)
    rows, feat = resid[0].shape
    chan = mixed[0].shape[1]
    width = feat * tp
    per = rows // tp
    return pl.pallas_call(
        functools.partial(mid_body, tp=tp),
        out_shape=(
            jax.ShapeDtypeStruct((per, width), bf16),
            jax.ShapeDtypeStruct((per, width), f32),
            jax.ShapeDtypeStruct((picked.shape[0], width), bf16),
        ),
        in_specs=[in_smem()] + [in_vmem()] * (2 * tp + 3),
        out_specs=(in_vmem(), in_hbm(), in_hbm()),
        scratch_shapes=[
            pltpu.VMEM((rows, chan * tp), bf16),
            pltpu.VMEM((rows, width), f32),
            pltpu.VMEM((rows, width), bf16),
            pltpu.VMEM((picked.shape[0], width), bf16),
            pltpu.SemaphoreType.DMA((2,)),
        ],
        compiler_params=pltpu.CompilerParams(vmem_limit_bytes=24 << 20),
        name="out_proj_norm",
    )(
        place,
        *resid,
        *mixed,
        weight,
        gain.reshape(1, width),
        picked,
    )


def join_body(*refs):
    parts, out, sems = refs[:-2], refs[-2], refs[-1]
    per = parts[0].shape[0]
    moves = [
        pltpu.make_async_copy(part, out.at[pl.ds(i * per, per), :], sems.at[i])
        for i, part in enumerate(parts)
    ]
    for copy in moves:
        copy.start()
    for copy in moves:
        copy.wait()


def join_kernel(parts):
    per, width = parts[0].shape
    return pl.pallas_call(
        join_body,
        out_shape=jax.ShapeDtypeStruct((per * len(parts), width), parts[0].dtype),
        in_specs=[in_vmem()] * len(parts),
        out_specs=in_hbm(),
        scratch_shapes=[pltpu.SemaphoreType.DMA((len(parts),))],
        compiler_params=pltpu.CompilerParams(vmem_limit_bytes=8 << 20),
        name="join_rows",
    )(*parts)


def tables_body(place, routes, weights, picked_out, share_out, *, experts, tp_count):
    top, rows = routes.shape
    slots = picked_out.shape[0]
    capacity = slots * tp_count // experts
    tp = place[0]
    chips = tp_count // cores
    per = rows // tp_count
    slot = lax.broadcasted_iota(jnp.int32, (slots, rows), 0)
    wanted = (slot // capacity) * tp_count + tp
    total = jnp.sum(weights[...], axis=0, keepdims=True)
    named = routes[0:1, :] == wanted
    share = jnp.where(named, weights[0:1, :] / total * routed_scale, 0.0)
    for j in range(1, top):
        hit = routes[j : j + 1, :] == wanted
        named = named | hit
        share = share + jnp.where(hit, weights[j : j + 1, :] / total * routed_scale, 0.0)
    down = lax.broadcasted_iota(jnp.int32, (rows, rows), 0)
    across = lax.broadcasted_iota(jnp.int32, (rows, rows), 1)
    rank = mm(named.astype(f32).astype(bf16), (down < across).astype(f32).astype(bf16))
    picked = named & (rank == (slot % capacity).astype(f32))
    picked_out[...] = jnp.where(picked, 1.0, 0.0).astype(bf16)
    share = jnp.where(picked, share, 0.0)
    high = share.astype(bf16)
    low = (share - high.astype(f32)).astype(bf16)
    ahead = (across // per) % chips
    core = (tp % cores) ^ (across // (per * chips))
    source = (((tp // cores + ahead) % chips) * cores + core) * per + across % per
    turn = (source == down).astype(f32).astype(bf16)
    share_out[:slots, :] = mm(high, turn).astype(bf16)
    share_out[slots:, :] = mm(low, turn).astype(bf16)


def tables_kernel(place, routes, weights, experts, tp_count):
    rows, top = routes.shape
    slots = max(2, 2 * rows * top // experts) * (experts // tp_count)
    return pl.pallas_call(
        functools.partial(tables_body, experts=experts, tp_count=tp_count),
        out_shape=(
            jax.ShapeDtypeStruct((slots, rows), bf16),
            jax.ShapeDtypeStruct((2 * slots, rows), bf16),
        ),
        in_specs=[in_smem()] + [in_vmem()] * 2,
        out_specs=(in_vmem(),) * 2,
        compiler_params=pltpu.CompilerParams(vmem_limit_bytes=8 << 20),
        name="slot_tables",
    )(place, routes.T, weights.T)


def layer(
    residual,
    in_gain,
    in_weight,
    state,
    decay_rate,
    frequency,
    log_step,
    in_coef,
    out_coef,
    skip_gain,
    out_weight,
    mid_gain,
    gate_vector,
    routes,
    route_weight,
    expert_gate,
    expert_up,
    expert_down,
    shared_gate,
    shared_up,
    shared_down,
):
    tp_count = lax.axis_size("tp")
    ep_count = lax.axis_size("ep")
    chips = tp_count // cores
    place = lax.axis_index("tp")
    seq_rows, feat_part = residual.shape
    width = feat_part * tp_count
    per_dev = seq_rows // tp_count
    capacity = max(2, 2 * seq_rows * routes.shape[1] // (ep_count * tp_count))
    slots = ep_count * capacity

    resid_mine, resid_other = hop_gather(residual, tp_count)
    own = (shared_gate, shared_up, shared_down)
    far = []
    for w, core in zip(own, (0, 1, 0)):
        far.append(lax.ppermute(w, ("ep", "tp"), weight_moves(ep_count, tp_count, core)))
    swap = [lax.ppermute(w, "tp", core_swap(tp_count)) for w in far]
    full_resid = natural_blocks(jnp.stack(resid_mine), jnp.stack(resid_other), tp_count, place).astype(f32)
    normed = layer_norm(full_resid, in_gain).astype(bf16)
    mixed_part, new_state = mixer_step(
        normed, in_weight, state, decay_rate, frequency, log_step, in_coef, out_coef, skip_gain
    )
    picked, share = tables_kernel(
        place.reshape(1), routes, route_weight, ep_count * tp_count, tp_count
    )
    mixed_mine, mixed_other = hop_gather(mixed_part, tp_count)
    out_rows = pull_kernel(out_weight)
    own_mid, own_after, outgoing = mid_kernel(
        place.reshape(1), resid_mine + resid_other, mixed_mine + mixed_other, out_rows, mid_gain, picked
    )

    side = math.isqrt(ep_count)
    line = [own_mid]
    for step in range(1, side):
        line.append(lax.ppermute(own_mid, "ep", plane_shift(ep_count, 0, step)))
    line = join_kernel(line)
    pair = lax.ppermute(line, "ep", pair_swap(ep_count))
    slot_rows = lax.all_to_all(
        outgoing.reshape(ep_count, capacity, width), "ep", split_axis=0, concat_axis=0, tiled=True
    ).reshape(slots, width)

    result = expert_kernel(slot_rows, expert_gate[0], expert_up[0], expert_down[0])
    returned = lax.all_to_all(
        result.reshape(ep_count, capacity, width), "ep", split_axis=0, concat_axis=0, tiled=True
    ).reshape(slots, width)

    group = 2 * side
    partial_rows = shared_kernel(
        lax.axis_index("ep").reshape(1), place.reshape(1), line, pair, own, far, swap, side
    )
    partial_back = lax.all_to_all(
        partial_rows.reshape(group, per_dev, width),
        "ep",
        split_axis=0,
        concat_axis=0,
        axis_index_groups=[list(range(g, g + group)) for g in range(0, ep_count, group)],
        tiled=True,
    )
    shared = jnp.sum(partial_back.astype(f32), axis=0)

    half = per_dev * chips
    doubled = jnp.concatenate([returned, returned], axis=0)
    send, keep = (
        lax.dot_general(
            part, doubled, (((0,), (0,)), ((), ())), preferred_element_type=f32
        ).astype(bf16)
        for part in (share[:, half:], share[:, :half])
    )
    theirs = lax.ppermute(send, "tp", core_swap(tp_count))
    pair = keep.astype(f32) + theirs.astype(f32)
    routed = pair[:per_dev]
    pair = pair.astype(bf16)
    for step in range(1, chips):
        piece = lax.ppermute(
            pair[step * per_dev : (step + 1) * per_dev], "tp", y_shift(tp_count, step)
        )
        routed = routed + piece.astype(f32)
    gate_value = jax.nn.sigmoid(jnp.dot(own_mid, gate_vector, preferred_element_type=f32))
    layer_out = (own_after + routed + gate_value[:, None] * shared).astype(bf16)
    return (layer_out, new_state)


def solution(mesh):
    return jax.shard_map(
        layer,
        mesh=mesh,
        in_specs=(
            P("ep", "tp"),
            P(),
            P(None, "tp"),
            P(None, "ep", "tp"),
            P("tp", None),
            P("tp", None),
            P("tp"),
            P(None, "tp", None, None),
            P(None, "tp", None, None),
            P("tp"),
            P(),
            P(),
            P(),
            P("ep", None),
            P("ep", None),
            P(("ep", "tp"), None, None),
            P(("ep", "tp"), None, None),
            P(("ep", "tp"), None, None),
            P(None, "ep"),
            P(None, "ep"),
            P("ep", None),
        ),
        out_specs=(P(("ep", "tp"), None), P(None, "ep", "tp")),
        check_vma=False,
    )
```
